32 devices in a mesh: grp: 2 (over y), sp: 4 (over z), tp: 4 (over x, core).
Axes of the slice: x: 2, y: 2, z: 4, core: 2. Of those that a mesh axis runs over, the one named last changes fastest.
Arguments:
- tokens: bfloat16 [3072, 4096], P(('grp', 'sp'), 'tp'), parts along dimension 0, may hold values from -6 to 6
- proj_b: bfloat16 [2, 4096, 2048], P(None, 'sp', 'tp'), may hold values from -0.09375 to 0.09375
- proj_c: bfloat16 [2, 4096, 2048], P(None, 'sp', 'tp'), may hold values from -0.09375 to 0.09375
- proj_x: bfloat16 [2, 4096, 2048], P(None, 'sp', 'tp'), may hold values from -0.09375 to 0.09375
- proj_out: bfloat16 [2, 2048, 4096], P(None, 'sp', 'tp'), may hold values from -1 to 1
- conv_taps: float32 [2, 3, 2048], P(None, None, 'tp'), may hold values from -3 to 3
- ln_gain: float32 [2, 4096], P(None, 'tp'), may hold values from 0.1 to 1.9
- ln_bias: float32 [2, 4096], P(None, 'tp'), may hold values from -2 to 2
Outputs:
- result: bfloat16 [3072, 4096], P(('grp', 'sp'), 'tp'), parts along dimension 0
The draws below stay inside these ranges and needn't reach their ends.
There are 2 independent parts, one for each index of `grp`. The reference program is written for one: setup_inputs(seed, part) draws one part's arguments, and reference() takes and returns one part's arrays. A program takes and returns all parts, laid end to end along the dimension named above; an argument that names none is the same for every part. Nothing has to cross between parts.
All inputs are finite; a program needn't handle non-finite values.
Results may differ from the reference program's by a relative error of at most 0.012.
Values may be sent and summed in bfloat16 or wider, within the bound.
A program may use at most 128 MiB of HBM per device.

```python
import jax
import jax.numpy as jnp
from jax import lax

D = 4096
CW = 2048
KW = 3
LAYERS = 2
TOKENS = 1536


def draw_proj_out(key, part):
    first_key = jax.random.fold_in(key, 11)
    second_key = jax.random.fold_in(key, 12)
    column_pos = jnp.arange(D, dtype=jnp.float32) / D
    jitter = jax.random.uniform(second_key, (LAYERS, 1, D), jnp.float32, -0.35, 0.35)
    entries = jax.random.normal(first_key, (LAYERS, CW, D), jnp.float32)
    ramp = jnp.exp(jnp.log(6.0) * column_pos)
    scaled = entries * CW ** (-0.5) * ramp * jnp.exp(jitter) / 2.5
    return jnp.clip(scaled, -1.0, 1.0).astype(jnp.bfloat16)


def block_levels(own_key, extent, shards, low, high):
    def one(dim, blocks):
        heights = jax.random.uniform(jax.random.fold_in(jax.random.fold_in(own_key, 6), dim), (blocks,), jnp.float32, low / len(shards), high / len(shards))
        return jnp.repeat(jnp.exp(heights), extent[dim] // blocks).reshape((-1,) + (1,) * (len(extent) - dim - 1))

    loudness = one(*shards[0])
    for cut in shards[1:]:
        loudness = loudness * one(*cut)
    return loudness


def centred(rng, shape, deviation, reach, split=(), held_as=jnp.bfloat16):
    factor_of = block_levels(rng, shape, split, -0.22, 0.18) if split else 1.0
    values = jax.random.normal(rng, shape, jnp.float32) * deviation * factor_of
    return jnp.minimum(jnp.maximum(values, -reach), reach).astype(held_as)


def setup_inputs(seed: int = 0, part: int = 0) -> dict:
    streams_of = jax.random.split(jax.random.key(seed), 9)
    part_keys = jax.random.split(jax.random.fold_in(streams_of[8], part), 9)
    tokens = centred(part_keys[0], (TOKENS, D), 1.0, 6.0, ((0, 4), (1, 4)))
    proj_b = centred(streams_of[1], (LAYERS, D, CW), D ** -0.5, 0.09375, ((1, 4), (2, 4)))
    proj_c = centred(streams_of[2], (LAYERS, D, CW), D ** -0.5, 0.09375, ((1, 4), (2, 4)))
    proj_x = centred(streams_of[3], (LAYERS, D, CW), D ** -0.5, 0.09375, ((1, 4), (2, 4)))
    proj_out = draw_proj_out(jax.random.fold_in(streams_of[8], 71), part)
    conv_taps = centred(streams_of[5], (LAYERS, KW, CW), 0.6, 3.0, ((2, 4),), jnp.float32)
    ln_gain = jnp.clip(1.0 + 0.18 * jax.random.normal(streams_of[6], (LAYERS, D), jnp.float32), 0.1, 1.9)
    ln_bias = centred(streams_of[7], (LAYERS, D), 0.3, 2.0, ((1, 4),), jnp.float32)
    return {"tokens": tokens, "proj_b": proj_b, "proj_c": proj_c, "proj_x": proj_x, "proj_out": proj_out, "conv_taps": conv_taps, "ln_gain": ln_gain, "ln_bias": ln_bias}


norm_eps = 1e-05

def reference(tokens, proj_b, proj_c, proj_x, proj_out, conv_taps, ln_gain, ln_bias):
    residual_scale = (2.0 * LAYERS) ** 0.25
    hidden = tokens
    for layer_index in range(LAYERS):
        out_gate = lax.optimization_barrier(jnp.dot(hidden, proj_b[layer_index], preferred_element_type=jnp.float32).astype(jnp.bfloat16))
        in_gate = lax.optimization_barrier(jnp.dot(hidden, proj_c[layer_index], preferred_element_type=jnp.float32).astype(jnp.bfloat16))
        values = lax.optimization_barrier(jnp.dot(hidden, proj_x[layer_index], preferred_element_type=jnp.float32).astype(jnp.bfloat16))
        gated_in = in_gate.astype(jnp.float32) * values.astype(jnp.float32)
        count_rows = gated_in.shape[0]
        padded = jnp.concatenate([jnp.zeros((KW - 1, gated_in.shape[1]), jnp.float32), gated_in], 0)
        conv_out = jnp.zeros_like(gated_in)
        for tap_index in range(KW):
            conv_out = conv_out + conv_taps[layer_index, tap_index] * padded[tap_index:tap_index + count_rows]
        branch = (out_gate.astype(jnp.float32) * conv_out).astype(jnp.bfloat16)
        mixed = lax.optimization_barrier(jnp.dot(branch, proj_out[layer_index], preferred_element_type=jnp.float32).astype(jnp.bfloat16))
        summed = residual_scale * hidden.astype(jnp.float32) + mixed.astype(jnp.float32)
        mean = lax.optimization_barrier(jnp.mean(summed, axis=1, keepdims=True))
        centered = summed - mean
        variance = lax.optimization_barrier(jnp.mean(centered * centered, axis=1, keepdims=True))
        hidden = (centered * lax.rsqrt(variance + norm_eps) * ln_gain[layer_index] + ln_bias[layer_index]).astype(jnp.bfloat16)
    return hidden
```

```python
import jax
import jax.numpy as jnp
from jax import lax
from jax.experimental import pallas as pl
from jax.experimental.pallas import tpu as pltpu
from jax.sharding import PartitionSpec as P


LAYERS = 2


norm_eps = 1e-05


def from_behind(block, axis, distance):
    devices = range(lax.axis_size(axis))
    route = [(i - distance, i) for i in devices if i - distance in devices]
    return lax.ppermute(block, axis, route)


def along_line(block, axis, earlier):
    size = lax.axis_size(axis)
    blocks, latest = [(0, block)], []
    for side, step in enumerate((1, -1)):
        moving = block
        if earlier:
            moving, _ = lax.optimization_barrier((moving, earlier[side]))
        hops = []
        for hop in range(1, size):
            start = range(hop - 1, size - 1) if step == 1 else range(1, size - hop + 1)
            moving = lax.ppermute(moving, axis, [(i, i + step) for i in start])
            hops.append((-step * hop, moving))
        latest.append(hops[max(len(hops) - 2, 0)][1])
        blocks += hops
    return sorted(blocks, key=lambda b: abs(b[0])), latest


def dot_by_blocks(left, blocks, here, size):
    total = None
    for offset, block in blocks:
        depth = block.shape[0]
        owner = jnp.clip(here + offset, 0, size - 1)
        columns = lax.dynamic_slice_in_dim(left, owner * depth, depth, 1)
        term = jnp.dot(columns, block, preferred_element_type=jnp.float32)
        total = term if total is None else total + term
    return total


def local(tokens, proj_b, proj_c, proj_x, proj_out, conv_taps, ln_gain, ln_bias):
    residual_scale = (2.0 * LAYERS) ** 0.25
    parts = lax.axis_size("grp")
    me = lax.axis_index("grp")
    rows = tokens.shape[0]
    wide = proj_b.shape[2] // parts
    out_wide = proj_out.shape[2] // parts

    def mine(array, width):
        return lax.dynamic_slice_in_dim(array, me * width, width, array.ndim - 1)

    slabs, here = lax.axis_size("sp"), lax.axis_index("sp")
    weights = []
    earlier = None
    for layer_index in range(LAYERS):
        ins = jnp.concatenate(
            [mine(w[layer_index], wide) for w in (proj_b, proj_c, proj_x)], axis=1
        )
        ins, earlier = along_line(ins, "sp", earlier)
        outs, earlier = along_line(mine(proj_out[layer_index], out_wide), "sp", earlier)
        weights.append((ins, outs))
    taps, gain, bias = mine(conv_taps, wide), mine(ln_gain, out_wide), mine(ln_bias, out_wide)
    swapped = lax.all_to_all(
        tokens.reshape(rows, parts, out_wide), "grp", split_axis=1, concat_axis=0, tiled=False
    )
    hidden = swapped.reshape(parts * rows, out_wide)
    reach = taps.shape[1] - 1
    for layer_index in range(LAYERS):
        whole_in, whole_out = weights[layer_index]
        gathered = lax.all_gather(hidden, ("tp", "grp"), axis=1, tiled=True)
        acc = dot_by_blocks(gathered, whole_in, here, slabs)
        acc = lax.optimization_barrier(acc.astype(jnp.bfloat16)).astype(jnp.float32)
        out_gate, in_gate, values = (acc[:, i * wide : (i + 1) * wide] for i in range(3))
        gated_in = (in_gate * values).reshape(parts, rows, wide)
        fringe = from_behind(gated_in[:, rows - reach :], "sp", 1)
        padded = jnp.concatenate([fringe, gated_in], 1)
        conv_out = jnp.zeros_like(gated_in)
        for tap_index in range(reach + 1):
            conv_out = (
                conv_out + taps[layer_index, tap_index] * padded[:, tap_index : tap_index + rows]
            )
        branch = (out_gate * conv_out.reshape(parts * rows, wide)).astype(jnp.bfloat16)
        all_branch = lax.all_gather(branch, ("tp", "grp"), axis=1, tiled=True)
        acc_out = dot_by_blocks(all_branch, whole_out, here, slabs)
        mixed = lax.optimization_barrier(acc_out.astype(jnp.bfloat16))
        summed = residual_scale * hidden.astype(jnp.float32) + mixed.astype(jnp.float32)
        own_mean = jnp.mean(summed, axis=1)
        own_spread = jnp.mean(jnp.square(summed - own_mean[:, None]), axis=1)
        stats = lax.all_gather(jnp.stack([own_mean, own_spread]), ("tp", "grp"), axis=0)
        mean = jnp.mean(stats[:, 0], axis=0)
        variance = jnp.mean(stats[:, 1] + jnp.square(stats[:, 0] - mean), axis=0)[:, None]
        centered = summed - mean[:, None]
        hidden = (
            centered * lax.rsqrt(variance + norm_eps) * gain[layer_index] + bias[layer_index]
        ).astype(jnp.bfloat16)
    back = lax.all_to_all(
        hidden.reshape(parts, rows, out_wide), "grp", split_axis=0, concat_axis=1, tiled=False
    )
    return back.reshape(rows, parts * out_wide)


MESH = pl.DeviceIdType.MESH
CHUNKS = 4
HALO = 32
VMEM_BYTES = 63 * 2**20


def multiple(value, of):
    return pl.multiple_of(value, of)


def tile_rows(rows, most):
    return max(n for n in range(16, most + 1, 16) if rows % n == 0)


def mixer_kernel(
    tokens, proj_b, proj_c, proj_x, proj_out, conv_taps, ln_gain, ln_bias, out,
    hidden, raw, branch, w_in, w_out, acc, carry, stage, final, scales, own_scales, stats,
    local_sem, w_send, w_recv, ag_send, ag_recv, small_send, small_recv,
):
    f32, bf16 = jnp.float32, jnp.bfloat16
    residual_scale = (2.0 * LAYERS) ** 0.25
    g, s, t = (lax.axis_index(a) for a in ("grp", "sp", "tp"))
    parts, _, lanes = (lax.axis_size(a) for a in ("grp", "sp", "tp"))
    x, c = t // 2, t % 2
    rows, ow = tokens.shape
    kin, kout = proj_b.shape[1], proj_out.shape[1]
    wide, owide = proj_b.shape[2] // parts, ow // parts
    reach = conv_taps.shape[1] - 1
    part_rows = HALO + 2 * rows
    chunk_rows = parts * part_rows // CHUNKS
    half = s // 2
    base, end, mid = 2 * half, 3 * half, 1 + half
    other, far = 2 - half, 3 - 3 * half
    projections = (proj_b, proj_c, proj_x)
    kc = kin // 2

    def copy(src, dst, send, recv, device):
        return pltpu.make_async_remote_copy(src, dst, send, recv, device_id=device, device_id_type=MESH)

    def piece(layer, block, k):
        if k == 2:
            return w_out.at[layer, pl.ds(multiple(block * kout, kout), kout), :]
        return w_in.at[layer, pl.ds(multiple(block * kin + k * kc, kc), kc), :]

    def send_own(layer, k, device, row):
        sems = (w_send.at[row, layer * 3 + k], w_recv.at[row, layer * 3 + k])
        if k == 2:
            src = proj_out.at[layer, :, pl.ds(multiple(g * owide, owide), owide)]
            copy(src, piece(layer, s, k), *sems, device).start()
        else:
            for j, w in enumerate(projections):
                src = w.at[layer, pl.ds(k * kc, kc), pl.ds(multiple(g * wide, wide), wide)]
                dst = w_in.at[layer, pl.ds(multiple(s * kin + k * kc, kc), kc), pl.ds(j * wide, wide)]
                copy(src, dst, *sems, device).start()

    def w_wait(layer, k, row, block, sent=False):
        ref = piece(layer, block, k)
        c_ = copy(ref, ref, w_send.at[row, layer * 3 + k], w_recv.at[row, layer * 3 + k], (g, s, t))
        c_.wait_send() if sent else c_.wait_recv()

    def relay(layer, k):
        w_wait(layer, k, 0, end)
        ref = piece(layer, end, k)
        copy(ref, ref, w_send.at[2, layer * 3 + k], w_recv.at[2, layer * 3 + k], (g, other, t)).start()

    pieces = [(layer, k) for layer in range(LAYERS) for k in range(3)]

    def token_rows(index):
        return pl.ds(multiple(g * part_rows + HALO + index * rows, 16), rows)

    own_columns = pl.ds(multiple(t * ow + g * owide, owide), owide)

    def final_half(gg):
        return final.at[:, pl.ds(multiple(gg * owide, owide), owide)]

    @pl.when(s == end)
    def _():
        slab = hidden.at[token_rows(end - base), pl.ds(multiple(t * ow, ow), ow)]
        copy(tokens, slab, small_send.at[0], small_recv.at[0], (g, mid, t)).start()
        for i, (layer, k) in enumerate(pieces):
            if i >= 2:
                w_wait(*pieces[i - 2], 0, s, sent=True)
            send_own(layer, k, (g, mid, t), 0)
        for layer, k in pieces[-2:]:
            w_wait(layer, k, 0, s, sent=True)
        copy(tokens, slab, small_send.at[0], small_recv.at[0], (g, mid, t)).wait_send()
        for gg in range(parts):
            copy(final_half(gg), final_half(gg), small_send.at[2], small_recv.at[8 + gg], (g, s, t)).wait_recv()

    @pl.when(s == mid)
    def _():
        there = (g, other, t)
        yu, xu = g + c * (1 - 2 * g), x + (1 - c) * (1 - 2 * x)
        yv, xv = g + (1 - c) * (1 - 2 * g), x + c * (1 - 2 * x)
        up, vp, pp = (yu, mid, 2 * xu + c), (yv, mid, 2 * xv + c), (g, mid, 2 * x + 1 - c)
        diagonal = (1 - g, mid, 2 * (1 - x) + c)
        me = (g, mid, t)

        for k in range(2):
            send_own(0, k, there, 1)
        mine = hidden.at[token_rows(mid - base), pl.ds(multiple(t * ow, ow), ow)]
        pltpu.make_async_copy(tokens, mine, local_sem.at[0]).start()
        for layer in range(LAYERS):
            for j, w in enumerate(projections):
                pltpu.make_async_copy(
                    w.at[layer, :, pl.ds(multiple(g * wide, wide), wide)],
                    w_in.at[layer, pl.ds(multiple(s * kin, kin), kin), pl.ds(j * wide, wide)],
                    local_sem.at[1 + layer],
                ).start()
            pltpu.make_async_copy(
                proj_out.at[layer, :, pl.ds(multiple(g * owide, owide), owide)],
                piece(layer, s, 2),
                local_sem.at[1 + LAYERS + layer],
            ).start()

        edge = hidden.at[pl.ds(multiple(g * part_rows, 16), HALO), pl.ds(multiple(t * ow, ow), ow)]
        edge_copy = copy(tokens.at[pl.ds(rows - HALO, HALO), :], edge, small_send.at[1], small_recv.at[1], there)

        @pl.when(half == 0)
        def _():
            edge_copy.start()
            edge[...] = jnp.zeros_like(edge)

        own_scales[0:1, :] = ln_gain[0:1, :]
        own_scales[1:2, :] = ln_bias[0:1, :]
        scales[0:2, pl.ds(multiple(t * ow, ow), ow)] = own_scales[0:2, :]
        for k in range(1, lanes):
            copy(
                own_scales, scales.at[:, pl.ds(multiple(t * ow, ow), ow)],
                small_send.at[4 + k], small_recv.at[4 + k], (g, s, (t + k) % lanes),
            ).start()

        def gather(buffer, region, family, produce, consume, unroll=False):
            def at(device, i):
                return buffer.at[region(device[0], device[2], i)]

            def transfer(owner, i, role, kind, device):
                ref = at(owner, i)
                return copy(ref, ref, ag_send.at[family, i, kind], ag_recv.at[family, i, role], device)

            def arrived(i, role):
                transfer(me, i, role, 0, me).wait_recv()

            def send(i):
                transfer(me, i, 0, 0, up).start()
                transfer(me, i, 1, 1, vp).start()
                transfer(me, i, 3, 2, pp).start()

            def step(i):
                arrived(i, 0)
                transfer(up, i, 2, 4, vp).start()
                transfer(up, i, 4, 3, pp).start()
                arrived(i, 1)
                transfer(vp, i, 5, 5, pp).start()
                arrived(i, 2)
                transfer(diagonal, i, 6, 6, pp).start()
                for role in range(3, 7):
                    arrived(i, role)
                consume(i)

            produce(0)
            send(0)
            if unroll:
                for i in range(CHUNKS):
                    if i + 1 < CHUNKS:
                        produce(i + 1)
                        send(i + 1)
                    step(i)
            else:
                @pl.loop(0, CHUNKS)
                def _(i):
                    @pl.when(i + 1 < CHUNKS)
                    def _():
                        produce(i + 1)
                        send(i + 1)

                    step(i)

            @pl.loop(0, CHUNKS)
            def _(i):
                for kind in range(7):
                    transfer(me, i, 0, kind, me).wait_send()

        def row_chunk(i):
            return pl.ds(multiple(i * chunk_rows, 16), chunk_rows)

        def nothing(i):
            pass

        def token_hook(i):
            if i in (1, 2):
                relay(0, i - 1)
            if i == 2:
                send_own(0, 2, there, 1)

        pltpu.make_async_copy(tokens, mine, local_sem.at[0]).wait()
        theirs = hidden.at[token_rows(end - base), pl.ds(multiple(t * ow, ow), ow)]
        copy(theirs, theirs, small_send.at[0], small_recv.at[0], me).wait_recv()

        @pl.when(half == 1)
        def _():
            edge_copy.wait_recv()

        qw = ow // CHUNKS
        gather(
            hidden,
            lambda gg, tt, i: (
                pl.ds(multiple(gg * part_rows, 16), part_rows),
                pl.ds(multiple(tt * ow + i * qw, qw), qw),
            ),
            0, nothing, token_hook, unroll=True,
        )

        def accumulate(layer, start, depth, i, first=False):
            at_rows = row_chunk(i)
            term = jnp.dot(
                hidden[at_rows, pl.ds(multiple(start, kc), depth)],
                w_in[layer, pl.ds(multiple(start, kc), depth), :],
                preferred_element_type=f32,
            )
            acc[at_rows, :] = term if first else acc[at_rows, :] + term

        def wait_near_in(layer):
            ref = w_in.at[layer, pl.ds(multiple(s * kin, kin), kin), :]
            pltpu.make_async_copy(ref, ref, local_sem.at[1 + layer]).wait()

        def near_in(layer, i):
            accumulate(layer, base * kin, 2 * kin, i, first=True)

        def far_in(layer):
            for row, block in ((1, other), (2, far)):
                for k in range(2):
                    w_wait(layer, k, row, block)

                    @pl.loop(0, CHUNKS)
                    def _(i):
                        accumulate(layer, block * kin + k * kc, kc, i)

        tr = tile_rows(chunk_rows, 96)

        def gate(layer, i):
            taps = [
                conv_taps[layer, k : k + 1, pl.ds(multiple(g * wide, wide), wide)] for k in range(reach + 1)
            ]
            row_of = lax.broadcasted_iota(jnp.int32, (tr, wide), 0)

            @pl.loop(0, chunk_rows // tr)
            def _(q):
                start = multiple(i * chunk_rows + q * tr, 16)
                position = start % part_rows
                sums = acc[pl.ds(start, tr), :].astype(bf16).astype(f32)
                out_gate, in_gate, values = (sums[:, j * wide : (j + 1) * wide] for j in range(3))
                gated = in_gate * values
                gated = jnp.where(row_of < HALO * (1 - half) - position, 0.0, gated)
                before = jnp.where(position == 0, 0.0, carry[...])
                conv = jnp.zeros_like(gated)
                for k in range(reach + 1):
                    shift = reach - k
                    moved = gated
                    if shift:
                        moved = pltpu.roll(gated, shift, 0)
                        for j in range(shift):
                            moved = jnp.where(row_of == j, before[8 - shift + j : 8 - shift + j + 1, :], moved)
                    conv = conv + taps[k] * moved
                carry[...] = gated[tr - 8 :, :]
                branch[pl.ds(start, tr), pl.ds(multiple(t * parts * wide + g * wide, wide), wide)] = (
                    out_gate * conv
                ).astype(bf16)

        def branch_region(gg, tt, i):
            return row_chunk(i), pl.ds(multiple(tt * parts * wide + gg * wide, wide), wide)

        def sum_region(gg, tt, i):
            return row_chunk(i), pl.ds(multiple(tt * ow + gg * owide, owide), owide)

        def wait_out(layer):
            ref = piece(layer, s, 2)
            pltpu.make_async_copy(ref, ref, local_sem.at[1 + LAYERS + layer]).wait()
            for row, block in ((1, other), (2, far)):
                w_wait(layer, 2, row, block)

        def mix(layer, at_rows):
            mixed = jnp.dot(branch[at_rows, :], w_out[layer], preferred_element_type=f32)
            kept = hidden[at_rows, own_columns].astype(f32)
            return (residual_scale * kept + mixed.astype(bf16).astype(f32)).astype(bf16)

        def produce_sum(i):
            raw[row_chunk(i), own_columns] = mix(0, row_chunk(i))

        def normalise(i):
            @pl.loop(0, chunk_rows // 16)
            def _(q):
                at_rows = pl.ds(multiple(i * chunk_rows + q * 16, 16), 16)
                summed = raw[at_rows, :].astype(f32)
                mean = jnp.mean(summed, axis=1, keepdims=True)
                centered = summed - mean
                variance = jnp.mean(centered * centered, axis=1, keepdims=True)
                hidden[at_rows, :] = (
                    centered * lax.rsqrt(variance + norm_eps) * scales[0:1, :] + scales[1:2, :]
                ).astype(bf16)

        def consume_sum(i):
            normalise(i)
            near_in(1, i)

        wait_near_in(0)

        @pl.loop(0, CHUNKS)
        def _(i):
            near_in(0, i)

        relay(0, 2)
        for k in range(2):
            send_own(1, k, there, 1)
        far_in(0)
        gather(branch, branch_region, 1, lambda i: gate(0, i), nothing)
        for k in range(2):
            relay(1, k)
        send_own(1, 2, there, 1)
        for k in range(1, lanes):
            copy(
                own_scales, scales.at[:, pl.ds(multiple(((t + lanes - k) % lanes) * ow, ow), ow)],
                small_send.at[4 + k], small_recv.at[4 + k], me,
            ).wait()
        wait_out(0)
        wait_near_in(1)
        gather(raw, sum_region, 0, produce_sum, consume_sum)
        relay(1, 2)
        far_in(1)
        gather(branch, branch_region, 1, lambda i: gate(1, i), nothing)
        wait_out(1)

        def result_copy(j):
            p = (g + 1 + j // 2) % 2
            to = end + (j % 2) * (mid - end)
            return p, to, copy(
                stage.at[j], final_half(g), small_send.at[12 + j], small_recv.at[8 + g], (p, to, t)
            )

        @pl.loop(0, 4)
        def _(j):
            p, to, result = result_copy(j)
            stage[j] = mix(1, pl.ds(multiple(p * part_rows + HALO + (to - base) * rows, 16), rows))

            @pl.when(j < 3)
            def _():
                result.start()

        final[:, pl.ds(multiple(g * owide, owide), owide)] = stage[3]
        for j in range(3):
            result_copy(j)[2].wait_send()
        for layer, k in pieces:
            w_wait(layer, k, 1, s, sent=True)
            w_wait(layer, k, 2, end, sent=True)

        @pl.when(half == 0)
        def _():
            edge_copy.wait_send()

        copy(final_half(1 - g), final_half(1 - g), small_send.at[2], small_recv.at[8 + 1 - g], me).wait_recv()

    lane = lax.broadcasted_iota(jnp.int32, (128, 128), 1)
    line = lax.broadcasted_iota(jnp.int32, (128, 128), 0)

    @pl.loop(0, rows // 128)
    def _(b):
        at_rows = pl.ds(multiple(b * 128, 128), 128)
        summed = final[at_rows, :].astype(f32)
        mean = jnp.mean(summed, axis=1, keepdims=True)
        spread = jnp.mean(jnp.square(summed - mean), axis=1, keepdims=True)
        packed = jnp.where(lane == 0, mean, jnp.where(lane == 1, spread, 0.0))
        stats[t, :, at_rows] = packed.T[0:8, :]

    def stat_copy(k, owner):
        return copy(
            stats.at[owner], stats.at[owner], small_send.at[4 + k], small_recv.at[16 + k], (g, s, (t + k) % lanes)
        )

    for k in range(1, lanes):
        stat_copy(k, t).start()
    for k in range(1, lanes):
        stat_copy(k, (t + lanes - k) % lanes).wait()

    @pl.loop(0, rows // 128)
    def _(b):
        at_rows = pl.ds(multiple(b * 128, 128), 128)
        means = [stats[i, 0:1, at_rows] for i in range(lanes)]
        mean = sum(means) / lanes
        variance = sum(stats[i, 1:2, at_rows] + jnp.square(means[i] - mean) for i in range(lanes)) / lanes
        packed = jnp.where(line == 0, mean, jnp.where(line == 1, lax.rsqrt(variance + norm_eps), 0.0)).T
        centered = final[at_rows, :].astype(f32) - packed[:, 0:1]
        out[at_rows, :] = (
            centered * packed[:, 1:2] * ln_gain[LAYERS - 1 : LAYERS, :] + ln_bias[LAYERS - 1 : LAYERS, :]
        ).astype(bf16)


def mixer(tokens, proj_b, proj_c, proj_x, proj_out, conv_taps, ln_gain, ln_bias):
    parts, slabs, lanes = (lax.axis_size(a) for a in ("grp", "sp", "tp"))
    f32, bf16 = jnp.float32, jnp.bfloat16
    rows, ow = tokens.shape
    depth, channels = slabs * proj_b.shape[1], slabs * proj_out.shape[1]
    wide, owide = proj_b.shape[2] // parts, ow // parts
    total = parts * (HALO + 2 * rows)
    dma = pltpu.SemaphoreType.DMA
    anywhere, vmem = pl.BlockSpec(memory_space=pl.ANY), pl.BlockSpec(memory_space=pltpu.VMEM)
    return pl.pallas_call(
        mixer_kernel,
        out_shape=jax.ShapeDtypeStruct((rows, ow), bf16),
        in_specs=[anywhere] * 5 + [vmem] * 3,
        out_specs=vmem,
        scratch_shapes=[
            pltpu.VMEM((total, depth), bf16),
            pltpu.VMEM((total, depth), bf16),
            pltpu.VMEM((total, channels), bf16),
            pltpu.VMEM((LAYERS, depth, 3 * wide), bf16),
            pltpu.VMEM((LAYERS, channels, owide), bf16),
            pltpu.VMEM((total, 3 * wide), f32),
            pltpu.VMEM((8, wide), f32),
            pltpu.VMEM((4, rows, owide), bf16),
            pltpu.VMEM((rows, ow), bf16),
            pltpu.VMEM((8, depth), f32),
            pltpu.VMEM((8, ow), f32),
            pltpu.VMEM((lanes, 8, rows), f32),
            dma((1 + 2 * LAYERS,)),
            dma((3, 3 * LAYERS)),
            dma((3, 3 * LAYERS)),
            dma((2, CHUNKS, 7)),
            dma((2, CHUNKS, 7)),
            dma((16,)),
            dma((20,)),
        ],
        compiler_params=pltpu.CompilerParams(has_side_effects=True, vmem_limit_bytes=VMEM_BYTES),
    )(tokens, proj_b, proj_c, proj_x, proj_out, conv_taps, ln_gain, ln_bias)


def solution(mesh):
    specs = dict(
        mesh=mesh,
        in_specs=(
            P(("grp", "sp"), "tp"),
            P(None, "sp", "tp"),
            P(None, "sp", "tp"),
            P(None, "sp", "tp"),
            P(None, "sp", "tp"),
            P(None, None, "tp"),
            P(None, "tp"),
            P(None, "tp"),
        ),
        out_specs=P(("grp", "sp"), "tp"),
        check_vma=False,
    )
    if (mesh.shape["grp"], mesh.shape["sp"], mesh.shape["tp"]) == (2, 4, 4):
        return jax.shard_map(mixer, **specs)
    return jax.shard_map(local, **specs)
```

```python
import jax
import jax.numpy as jnp
from jax import lax
from jax.experimental import pallas as pl
from jax.experimental.pallas import tpu as pltpu
from jax.sharding import PartitionSpec as P


LAYERS = 2


norm_eps = 1e-05


def from_behind(block, axis, distance):
    devices = range(lax.axis_size(axis))
    route = [(i - distance, i) for i in devices if i - distance in devices]
    return lax.ppermute(block, axis, route)


def along_line(block, axis, earlier):
    size = lax.axis_size(axis)
    blocks, latest = [(0, block)], []
    for side, step in enumerate((1, -1)):
        moving = block
        if earlier:
            moving, _ = lax.optimization_barrier((moving, earlier[side]))
        hops = []
        for hop in range(1, size):
            start = range(hop - 1, size - 1) if step == 1 else range(1, size - hop + 1)
            moving = lax.ppermute(moving, axis, [(i, i + step) for i in start])
            hops.append((-step * hop, moving))
        latest.append(hops[max(len(hops) - 2, 0)][1])
        blocks += hops
    return sorted(blocks, key=lambda b: abs(b[0])), latest


def dot_by_blocks(left, blocks, here, size):
    total = None
    for offset, block in blocks:
        depth = block.shape[0]
        owner = jnp.clip(here + offset, 0, size - 1)
        columns = lax.dynamic_slice_in_dim(left, owner * depth, depth, 1)
        term = jnp.dot(columns, block, preferred_element_type=jnp.float32)
        total = term if total is None else total + term
    return total


def local(tokens, proj_b, proj_c, proj_x, proj_out, conv_taps, ln_gain, ln_bias):
    residual_scale = (2.0 * LAYERS) ** 0.25
    parts = lax.axis_size("grp")
    me = lax.axis_index("grp")
    rows = tokens.shape[0]
    wide = proj_b.shape[2] // parts
    out_wide = proj_out.shape[2] // parts

    def mine(array, width):
        return lax.dynamic_slice_in_dim(array, me * width, width, array.ndim - 1)

    slabs, here = lax.axis_size("sp"), lax.axis_index("sp")
    weights = []
    earlier = None
    for layer_index in range(LAYERS):
        ins = jnp.concatenate(
            [mine(w[layer_index], wide) for w in (proj_b, proj_c, proj_x)], axis=1
        )
        ins, earlier = along_line(ins, "sp", earlier)
        outs, earlier = along_line(mine(proj_out[layer_index], out_wide), "sp", earlier)
        weights.append((ins, outs))
    taps, gain, bias = mine(conv_taps, wide), mine(ln_gain, out_wide), mine(ln_bias, out_wide)
    swapped = lax.all_to_all(
        tokens.reshape(rows, parts, out_wide), "grp", split_axis=1, concat_axis=0, tiled=False
    )
    hidden = swapped.reshape(parts * rows, out_wide)
    reach = taps.shape[1] - 1
    for layer_index in range(LAYERS):
        whole_in, whole_out = weights[layer_index]
        gathered = lax.all_gather(hidden, ("tp", "grp"), axis=1, tiled=True)
        acc = dot_by_blocks(gathered, whole_in, here, slabs)
        acc = lax.optimization_barrier(acc.astype(jnp.bfloat16)).astype(jnp.float32)
        out_gate, in_gate, values = (acc[:, i * wide : (i + 1) * wide] for i in range(3))
        gated_in = (in_gate * values).reshape(parts, rows, wide)
        fringe = from_behind(gated_in[:, rows - reach :], "sp", 1)
        padded = jnp.concatenate([fringe, gated_in], 1)
        conv_out = jnp.zeros_like(gated_in)
        for tap_index in range(reach + 1):
            conv_out = (
                conv_out + taps[layer_index, tap_index] * padded[:, tap_index : tap_index + rows]
            )
        branch = (out_gate * conv_out.reshape(parts * rows, wide)).astype(jnp.bfloat16)
        all_branch = lax.all_gather(branch, ("tp", "grp"), axis=1, tiled=True)
        acc_out = dot_by_blocks(all_branch, whole_out, here, slabs)
        mixed = lax.optimization_barrier(acc_out.astype(jnp.bfloat16))
        summed = residual_scale * hidden.astype(jnp.float32) + mixed.astype(jnp.float32)
        own_mean = jnp.mean(summed, axis=1)
        own_spread = jnp.mean(jnp.square(summed - own_mean[:, None]), axis=1)
        stats = lax.all_gather(jnp.stack([own_mean, own_spread]), ("tp", "grp"), axis=0)
        mean = jnp.mean(stats[:, 0], axis=0)
        variance = jnp.mean(stats[:, 1] + jnp.square(stats[:, 0] - mean), axis=0)[:, None]
        centered = summed - mean[:, None]
        hidden = (
            centered * lax.rsqrt(variance + norm_eps) * gain[layer_index] + bias[layer_index]
        ).astype(jnp.bfloat16)
    back = lax.all_to_all(
        hidden.reshape(parts, rows, out_wide), "grp", split_axis=0, concat_axis=1, tiled=False
    )
    return back.reshape(rows, parts * out_wide)


MESH = pl.DeviceIdType.MESH
CHUNKS = 4
HALO = 32
VMEM_BYTES = 63 * 2**20


def multiple(value, of):
    return pl.multiple_of(value, of)


def tile_rows(rows, most):
    return max(n for n in range(16, most + 1, 16) if rows % n == 0)


def mixer_kernel(
    tokens, proj_b, proj_c, proj_x, proj_out, conv_taps, ln_gain, ln_bias, out,
    hidden, raw, branch, w_in, w_out, acc, carry, stage, final, scales, own_scales, stats, ones, means,
    local_sem, w_send, w_recv, ag_send, ag_recv, small_send, small_recv,
):
    f32, bf16 = jnp.float32, jnp.bfloat16
    residual_scale = (2.0 * LAYERS) ** 0.25
    g, s, t = (lax.axis_index(a) for a in ("grp", "sp", "tp"))
    parts, _, lanes = (lax.axis_size(a) for a in ("grp", "sp", "tp"))
    x, c = t // 2, t % 2
    rows, ow = tokens.shape
    kin, kout = proj_b.shape[1], proj_out.shape[1]
    wide, owide = proj_b.shape[2] // parts, ow // parts
    reach = conv_taps.shape[0] - 1
    part_rows = HALO + 2 * rows
    chunk_rows = parts * part_rows // CHUNKS
    half = s // 2
    base, end, mid = 2 * half, 3 * half, 1 + half
    other, far = 2 - half, 3 - 3 * half
    projections = (proj_b, proj_c, proj_x)
    sub = wide // 2
    pieces_in, pieces = (0, 1), 3

    def copy(src, dst, send, recv, device):
        return pltpu.make_async_remote_copy(src, dst, send, recv, device_id=device, device_id_type=MESH)

    def piece(layer, block, k):
        if k in pieces_in:
            return w_in.at[layer, k, pl.ds(multiple(block * kin, kin), kin), :]
        return w_out.at[layer, pl.ds(multiple(block * kout, kout), kout), :]

    def piece_parts(layer, k):
        if k in pieces_in:
            columns = pl.ds(multiple(g * wide + k * sub, sub), sub)
            rows_there = pl.ds(multiple(s * kin, kin), kin)
            for j, w in enumerate(projections):
                yield w.at[layer, :, columns], w_in.at[layer, k, rows_there, pl.ds(j * sub, sub)]
        else:
            columns = pl.ds(multiple(g * owide, owide), owide)
            yield proj_out.at[layer, :, columns], piece(layer, s, k)

    def send_own(layer, k, device, row):
        sems = (w_send.at[row, layer * pieces + k], w_recv.at[row, layer * pieces + k])
        for src, dst in piece_parts(layer, k):
            copy(src, dst, *sems, device).start()

    def w_wait(layer, k, row, block, sent=False):
        ref = piece(layer, block, k)
        done = copy(ref, ref, w_send.at[row, layer * pieces + k], w_recv.at[row, layer * pieces + k], (g, s, t))
        done.wait_send() if sent else done.wait_recv()

    def relay(layer, k):
        w_wait(layer, k, 0, end)
        ref = piece(layer, end, k)
        sems = (w_send.at[2, layer * pieces + k], w_recv.at[2, layer * pieces + k])
        copy(ref, ref, *sems, (g, other, t)).start()

    order = [(layer, k) for layer in range(LAYERS) for k in range(pieces)]

    def token_rows(index):
        return pl.ds(multiple(g * part_rows + HALO + index * rows, 16), rows)

    def final_part(gg):
        return final.at[:, pl.ds(multiple(gg * owide, owide), owide)]

    def final_arrived(gg):
        ref = final_part(gg)
        copy(ref, ref, small_send.at[2], small_recv.at[8 + gg], (g, s, t)).wait_recv()

    barrier = pltpu.get_barrier_semaphore()

    def greet(devices):
        for device in devices:
            pl.semaphore_signal(barrier, inc=1, device_id=device, device_id_type=MESH)
        pl.semaphore_wait(barrier, len(devices))

    lane_peers = [(g, s, (t + k) % lanes) for k in range(1, lanes)]

    def end_slab(j):
        start = multiple(g * part_rows + HALO + (end - base) * rows + j * (rows // 2), 16)
        return hidden.at[pl.ds(start, rows // 2), pl.ds(multiple(t * ow, ow), ow)]

    def end_tokens(j):
        return copy(
            tokens.at[pl.ds(j * (rows // 2), rows // 2), :], end_slab(j),
            small_send.at[3 * j], small_recv.at[3 * j], (g, mid, t),
        )

    @pl.when(s == end)
    def _():
        greet(lane_peers + [(gg, mid, t) for gg in range(parts)])
        for j in range(2):
            end_tokens(j).start()
        for j in range(2):
            end_tokens(j).wait_send()
        for layer, k in order:
            send_own(layer, k, (g, mid, t), 0)
            w_wait(layer, k, 0, s, sent=True)
        for gg in range(parts):
            final_arrived(gg)

    @pl.when(s == mid)
    def _():
        there = (g, other, t)
        yu, xu = g + c * (1 - 2 * g), x + (1 - c) * (1 - 2 * x)
        yv, xv = g + (1 - c) * (1 - 2 * g), x + c * (1 - 2 * x)
        up, vp, pp = (yu, mid, 2 * xu + c), (yv, mid, 2 * xv + c), (g, mid, 2 * x + 1 - c)
        diagonal = (1 - g, mid, 2 * (1 - x) + c)
        me = (g, mid, t)

        greet(lane_peers + [(1 - g, mid, t), there] + [(gg, end, t) for gg in range(parts)])
        send_own(0, 0, there, 1)
        mine = hidden.at[token_rows(mid - base), pl.ds(multiple(t * ow, ow), ow)]
        pltpu.make_async_copy(tokens, mine, local_sem.at[0]).start()
        for layer, k in order:
            for src, dst in piece_parts(layer, k):
                pltpu.make_async_copy(src, dst, local_sem.at[1 + layer * pieces + k]).start()

        edge = hidden.at[pl.ds(multiple(g * part_rows, 16), HALO), pl.ds(multiple(t * ow, ow), ow)]
        edge_copy = copy(tokens.at[pl.ds(rows - HALO, HALO), :], edge, small_send.at[1], small_recv.at[1], there)

        @pl.when(half == 0)
        def _():
            edge_copy.start()
            edge[...] = jnp.zeros_like(edge)

        own_scales[0:1, :] = ln_gain[0:1, :]
        own_scales[1:2, :] = ln_bias[0:1, :]
        scales[0:2, pl.ds(multiple(t * ow, ow), ow)] = own_scales[0:2, :]
        for k in range(1, lanes):
            copy(
                own_scales, scales.at[:, pl.ds(multiple(t * ow, ow), ow)],
                small_send.at[4 + k], small_recv.at[4 + k], (g, s, (t + k) % lanes),
            ).start()

        def gather(buffer, region, count, family, produce, consume, ahead, unroll=False):
            def at(device, i):
                return buffer.at[region(device[0], device[2], i)]

            def transfer(owner, i, role, kind, device):
                ref = at(owner, i)
                return copy(ref, ref, ag_send.at[family, i, kind], ag_recv.at[family, i, role], device)

            def arrived(i, role):
                transfer(me, i, role, 0, me).wait_recv()

            def send(i):
                produce(i)
                transfer(me, i, 0, 0, up).start()
                transfer(me, i, 1, 1, vp).start()
                transfer(me, i, 3, 2, pp).start()

            def pass_on(i):
                arrived(i, 0)
                transfer(up, i, 2, 4, vp).start()
                transfer(up, i, 4, 3, pp).start()
                arrived(i, 1)
                transfer(vp, i, 5, 5, pp).start()

            def finish(i):
                arrived(i, 2)
                transfer(diagonal, i, 6, 6, pp).start()
                for role in range(3, 7):
                    arrived(i, role)
                consume(i)

            def sent(i):
                for kind in range(7):
                    transfer(me, i, 0, kind, me).wait_send()

            for i in range(ahead):
                send(i)
            if unroll:
                for i in range(count + 1):
                    if i + ahead < count:
                        send(i + ahead)
                    if i < count:
                        pass_on(i)
                    if i:
                        finish(i - 1)
                for i in range(count):
                    sent(i)
            else:
                @pl.loop(0, count + 1)
                def _(i):
                    @pl.when(i + ahead < count)
                    def _():
                        send(i + ahead)

                    @pl.when(i < count)
                    def _():
                        pass_on(i)

                    @pl.when(i > 0)
                    def _():
                        finish(i - 1)

                @pl.loop(0, count)
                def _(i):
                    sent(i)

        def row_chunk(i):
            return pl.ds(multiple(i * chunk_rows, 16), chunk_rows)

        def nothing(i):
            pass

        first_half = rows // 2
        token_starts = (
            HALO + (mid - base) * rows,
            HALO + (mid - base) * rows + first_half,
            0,
            HALO + (end - base) * rows,
            HALO + (end - base) * rows + first_half,
        )

        def token_region(gg, tt, i):
            length = HALO if i == 2 else first_half
            return (
                pl.ds(multiple(gg * part_rows + token_starts[i], 16), length),
                pl.ds(multiple(tt * ow, ow), ow),
            )

        def token_ready(i):
            if i == 0:
                pltpu.make_async_copy(tokens, mine, local_sem.at[0]).wait()
            if i == 2:
                @pl.when(half == 1)
                def _():
                    edge_copy.wait_recv()
            if i > 2:
                slab = end_slab(i - 3)
                copy(slab, slab, small_send.at[3 * (i - 3)], small_recv.at[3 * (i - 3)], me).wait_recv()

        def token_hook(i):
            if i == 0:
                send_own(0, 1, there, 1)
            if i == 3:
                relay(0, 0)
            if i == 4:
                relay(0, 1)

        gather(hidden, token_region, 5, 0, token_ready, token_hook, 2, unroll=True)

        def accumulate(layer, k, start, depth, i, first=False):
            at_rows = row_chunk(i)
            term = jnp.dot(
                hidden[at_rows, pl.ds(multiple(start, kin), depth)],
                w_in[layer, k, pl.ds(multiple(start, kin), depth), :],
                preferred_element_type=f32,
            )
            acc[k, at_rows, :] = term if first else acc[k, at_rows, :] + term

        def wait_near(layer, k):
            ref = piece(layer, s, k)
            pltpu.make_async_copy(ref, ref, local_sem.at[1 + layer * pieces + k]).wait()

        def near_in(layer, k, i):
            accumulate(layer, k, base * kin, 2 * kin, i, first=True)

        def far_in(layer, k):
            for row, block in ((1, other), (2, far)):
                w_wait(layer, k, row, block)

            @pl.loop(0, CHUNKS)
            def _(i):
                accumulate(layer, k, 2 * (1 - half) * kin, 2 * kin, i)

        tr = tile_rows(chunk_rows, 96)

        def branch_columns(gg, tt, k):
            return pl.ds(multiple(tt * parts * wide + gg * wide + k * sub, sub), sub)

        def gate(layer, k, i):
            taps = [
                conv_taps[n, layer : layer + 1, pl.ds(multiple(g * wide + k * sub, sub), sub)] for n in range(reach + 1)
            ]
            row_of = lax.broadcasted_iota(jnp.int32, (tr, sub), 0)

            @pl.loop(0, chunk_rows // tr)
            def _(q):
                start = multiple(i * chunk_rows + q * tr, 16)
                position = start % part_rows
                sums = acc[k, pl.ds(start, tr), :].astype(bf16).astype(f32)
                out_gate, in_gate, values = (sums[:, j * sub : (j + 1) * sub] for j in range(3))
                gated = in_gate * values
                gated = jnp.where(row_of < HALO * (1 - half) - position, 0.0, gated)
                before = jnp.where(position == 0, 0.0, carry[...])
                conv = jnp.zeros_like(gated)
                for n in range(reach + 1):
                    shift = reach - n
                    moved = gated
                    if shift:
                        moved = pltpu.roll(gated, shift, 0)
                        for j in range(shift):
                            moved = jnp.where(row_of == j, before[8 - shift + j : 8 - shift + j + 1, :], moved)
                    conv = conv + taps[n] * moved
                carry[...] = gated[tr - 8 :, :]
                branch[pl.ds(start, tr), branch_columns(g, t, k)] = (out_gate * conv).astype(bf16)

        def branches(layer, k, consume):
            gather(
                branch, lambda gg, tt, i: (row_chunk(i), branch_columns(gg, tt, k)),
                CHUNKS, 1 + k, lambda i: gate(layer, k, i), consume, 2,
            )

        def sum_region(gg, tt, i):
            return row_chunk(i), pl.ds(multiple(tt * ow + gg * owide, owide), owide)

        def wait_out(layer):
            wait_near(layer, 2)
            for row, block in ((1, other), (2, far)):
                w_wait(layer, 2, row, block)

        own_columns = pl.ds(multiple(t * ow + g * owide, owide), owide)

        def mix(layer, at_rows):
            mixed = jnp.dot(branch[at_rows, :], w_out[layer], preferred_element_type=f32)
            kept = hidden[at_rows, own_columns].astype(f32)
            return (residual_scale * kept + mixed.astype(bf16).astype(f32)).astype(bf16)

        def produce_sum(i):
            raw[row_chunk(i), own_columns] = mix(0, row_chunk(i))

        strips = [slice(n, n + 128) for n in range(0, hidden.shape[1], 128)]
        ones[...] = jnp.ones_like(ones)

        def normalise(i):
            means[...] = jnp.dot(raw[row_chunk(i), :], ones[...], preferred_element_type=f32) / ones.shape[0]

            @pl.loop(0, chunk_rows // tr)
            def _(q):
                there_rows = pl.ds(multiple(i * chunk_rows + q * tr, 16), tr)
                here_rows = pl.ds(multiple(q * tr, 16), tr)
                mean = means[here_rows, :]
                total = jnp.zeros_like(mean)
                for strip in strips:
                    centered = raw[there_rows, strip].astype(f32) - mean
                    total = total + centered * centered
                scale = lax.rsqrt(jnp.sum(total, axis=1, keepdims=True) / ones.shape[0] + norm_eps)
                scale = jnp.broadcast_to(scale, mean.shape)
                for strip in strips:
                    centered = raw[there_rows, strip].astype(f32) - mean
                    hidden[there_rows, strip] = (
                        centered * scale * scales[0:1, strip] + scales[1:2, strip]
                    ).astype(bf16)

        def send_pair(layer, k):
            send_own(layer, k, there, 1)
            relay(layer, k)

        def consume_sum(i):
            normalise(i)
            near_in(1, 0, i)

            @pl.when(i == 0)
            def _():
                send_pair(1, 1)

            near_in(1, 1, i)

        def first_branches(i):
            near_in(0, 1, i)

            @pl.when(i == CHUNKS - 1)
            def _():
                send_pair(0, 2)

        for k in pieces_in:
            wait_near(0, k)

        @pl.loop(0, CHUNKS)
        def _(i):
            near_in(0, 0, i)

        far_in(0, 0)
        branches(0, 0, first_branches)
        far_in(0, 1)
        branches(0, 1, nothing)
        send_pair(1, 0)
        for k in range(1, lanes):
            copy(
                own_scales, scales.at[:, pl.ds(multiple(((t + lanes - k) % lanes) * ow, ow), ow)],
                small_send.at[4 + k], small_recv.at[4 + k], me,
            ).wait()
        wait_out(0)
        for k in pieces_in:
            wait_near(1, k)
        gather(raw, sum_region, CHUNKS, 0, produce_sum, consume_sum, 1)
        far_in(1, 0)
        send_pair(1, 2)
        branches(1, 0, nothing)
        far_in(1, 1)
        branches(1, 1, nothing)
        wait_out(1)

        def result_copy(j):
            p = (g + 1 + j // 2) % 2
            to = end + (j % 2) * (mid - end)
            return p, to, copy(
                stage.at[j], final_part(g), small_send.at[12 + j], small_recv.at[8 + g], (p, to, t)
            )

        @pl.loop(0, 4)
        def _(j):
            p, to, result = result_copy(j)
            stage[j] = mix(1, pl.ds(multiple(p * part_rows + HALO + (to - base) * rows, 16), rows))

            @pl.when(j < 3)
            def _():
                result.start()

        final[:, pl.ds(multiple(g * owide, owide), owide)] = stage[3]
        for j in range(3):
            result_copy(j)[2].wait_send()
        for layer, k in order:
            w_wait(layer, k, 1, s, sent=True)
            w_wait(layer, k, 2, end, sent=True)

        @pl.when(half == 0)
        def _():
            edge_copy.wait_send()

        final_arrived(1 - g)

    lane = lax.broadcasted_iota(jnp.int32, (128, 128), 1)
    line = lax.broadcasted_iota(jnp.int32, (128, 128), 0)

    @pl.loop(0, rows // 128)
    def _(b):
        at_rows = pl.ds(multiple(b * 128, 128), 128)
        summed = final[at_rows, :].astype(f32)
        mean = jnp.mean(summed, axis=1, keepdims=True)
        spread = jnp.mean(jnp.square(summed - mean), axis=1, keepdims=True)
        packed = jnp.where(lane == 0, mean, jnp.where(lane == 1, spread, 0.0))
        stats[t, :, at_rows] = packed.T[0:8, :]

    def stat_copy(k, owner):
        return copy(
            stats.at[owner], stats.at[owner], small_send.at[4 + k], small_recv.at[16 + k], (g, s, (t + k) % lanes)
        )

    for k in range(1, lanes):
        stat_copy(k, t).start()
    for k in range(1, lanes):
        stat_copy(k, (t + lanes - k) % lanes).wait()

    @pl.loop(0, rows // 128)
    def _(b):
        at_rows = pl.ds(multiple(b * 128, 128), 128)
        means = [stats[i, 0:1, at_rows] for i in range(lanes)]
        mean = sum(means) / lanes
        variance = sum(stats[i, 1:2, at_rows] + jnp.square(means[i] - mean) for i in range(lanes)) / lanes
        packed = jnp.where(line == 0, mean, jnp.where(line == 1, lax.rsqrt(variance + norm_eps), 0.0)).T
        centered = final[at_rows, :].astype(f32) - packed[:, 0:1]
        out[at_rows, :] = (
            centered * packed[:, 1:2] * ln_gain[LAYERS - 1 : LAYERS, :] + ln_bias[LAYERS - 1 : LAYERS, :]
        ).astype(bf16)


def mixer(tokens, proj_b, proj_c, proj_x, proj_out, conv_taps, ln_gain, ln_bias):
    parts, slabs, lanes = (lax.axis_size(a) for a in ("grp", "sp", "tp"))
    f32, bf16 = jnp.float32, jnp.bfloat16
    rows, ow = tokens.shape
    depth, channels = slabs * proj_b.shape[1], slabs * proj_out.shape[1]
    wide, owide = proj_b.shape[2] // parts, ow // parts
    total = parts * (HALO + 2 * rows)
    dma = pltpu.SemaphoreType.DMA
    anywhere, vmem = pl.BlockSpec(memory_space=pl.ANY), pl.BlockSpec(memory_space=pltpu.VMEM)
    return pl.pallas_call(
        mixer_kernel,
        out_shape=jax.ShapeDtypeStruct((rows, ow), bf16),
        in_specs=[anywhere] * 5 + [vmem] * 3,
        out_specs=vmem,
        scratch_shapes=[
            pltpu.VMEM((total, depth), bf16),
            pltpu.VMEM((total, depth), bf16),
            pltpu.VMEM((total, channels), bf16),
            pltpu.VMEM((LAYERS, 2, depth, 3 * wide // 2), bf16),
            pltpu.VMEM((LAYERS, channels, owide), bf16),
            pltpu.VMEM((2, total, 3 * wide // 2), f32),
            pltpu.VMEM((8, wide // 2), f32),
            pltpu.VMEM((4, rows, owide), bf16),
            pltpu.VMEM((rows, ow), bf16),
            pltpu.VMEM((8, depth), f32),
            pltpu.VMEM((8, ow), f32),
            pltpu.VMEM((lanes, 8, rows), f32),
            pltpu.VMEM((depth, 128), bf16),
            pltpu.VMEM((total // CHUNKS, 128), f32),
            dma((1 + 3 * LAYERS,)),
            dma((3, 3 * LAYERS)),
            dma((3, 3 * LAYERS)),
            dma((3, 5, 7)),
            dma((3, 5, 7)),
            dma((20,)),
            dma((20,)),
        ],
        compiler_params=pltpu.CompilerParams(
            has_side_effects=True, collective_id=0, vmem_limit_bytes=VMEM_BYTES
        ),
    )(tokens, proj_b, proj_c, proj_x, proj_out, conv_taps.transpose(1, 0, 2), ln_gain, ln_bias)


def solution(mesh):
    specs = dict(
        mesh=mesh,
        in_specs=(
            P(("grp", "sp"), "tp"),
            P(None, "sp", "tp"),
            P(None, "sp", "tp"),
            P(None, "sp", "tp"),
            P(None, "sp", "tp"),
            P(None, None, "tp"),
            P(None, "tp"),
            P(None, "tp"),
        ),
        out_specs=P(("grp", "sp"), "tp"),
        check_vma=False,
    )
    if (mesh.shape["grp"], mesh.shape["sp"], mesh.shape["tp"]) == (2, 4, 4):
        return jax.shard_map(mixer, **specs)
    return jax.shard_map(local, **specs)
```

```python
import jax
import jax.numpy as jnp
from jax import lax
from jax.experimental import pallas as pl
from jax.experimental.pallas import tpu as pltpu
from jax.sharding import PartitionSpec as P


LAYERS = 2


norm_eps = 1e-05


def from_behind(block, axis, distance):
    devices = range(lax.axis_size(axis))
    route = [(i - distance, i) for i in devices if i - distance in devices]
    return lax.ppermute(block, axis, route)


def along_line(block, axis, earlier):
    size = lax.axis_size(axis)
    blocks, latest = [(0, block)], []
    for side, step in enumerate((1, -1)):
        moving = block
        if earlier:
            moving, _ = lax.optimization_barrier((moving, earlier[side]))
        hops = []
        for hop in range(1, size):
            start = range(hop - 1, size - 1) if step == 1 else range(1, size - hop + 1)
            moving = lax.ppermute(moving, axis, [(i, i + step) for i in start])
            hops.append((-step * hop, moving))
        latest.append(hops[max(len(hops) - 2, 0)][1])
        blocks += hops
    return sorted(blocks, key=lambda b: abs(b[0])), latest


def dot_by_blocks(left, blocks, here, size):
    total = None
    for offset, block in blocks:
        depth = block.shape[0]
        owner = jnp.clip(here + offset, 0, size - 1)
        columns = lax.dynamic_slice_in_dim(left, owner * depth, depth, 1)
        term = jnp.dot(columns, block, preferred_element_type=jnp.float32)
        total = term if total is None else total + term
    return total


def local(tokens, proj_b, proj_c, proj_x, proj_out, conv_taps, ln_gain, ln_bias):
    residual_scale = (2.0 * LAYERS) ** 0.25
    parts = lax.axis_size("grp")
    me = lax.axis_index("grp")
    rows = tokens.shape[0]
    wide = proj_b.shape[2] // parts
    out_wide = proj_out.shape[2] // parts

    def mine(array, width):
        return lax.dynamic_slice_in_dim(array, me * width, width, array.ndim - 1)

    slabs, here = lax.axis_size("sp"), lax.axis_index("sp")
    weights = []
    earlier = None
    for layer_index in range(LAYERS):
        ins = jnp.concatenate(
            [mine(w[layer_index], wide) for w in (proj_b, proj_c, proj_x)], axis=1
        )
        ins, earlier = along_line(ins, "sp", earlier)
        outs, earlier = along_line(mine(proj_out[layer_index], out_wide), "sp", earlier)
        weights.append((ins, outs))
    taps, gain, bias = mine(conv_taps, wide), mine(ln_gain, out_wide), mine(ln_bias, out_wide)
    swapped = lax.all_to_all(
        tokens.reshape(rows, parts, out_wide), "grp", split_axis=1, concat_axis=0, tiled=False
    )
    hidden = swapped.reshape(parts * rows, out_wide)
    reach = taps.shape[1] - 1
    for layer_index in range(LAYERS):
        whole_in, whole_out = weights[layer_index]
        gathered = lax.all_gather(hidden, ("tp", "grp"), axis=1, tiled=True)
        acc = dot_by_blocks(gathered, whole_in, here, slabs)
        acc = lax.optimization_barrier(acc.astype(jnp.bfloat16)).astype(jnp.float32)
        out_gate, in_gate, values = (acc[:, i * wide : (i + 1) * wide] for i in range(3))
        gated_in = (in_gate * values).reshape(parts, rows, wide)
        fringe = from_behind(gated_in[:, rows - reach :], "sp", 1)
        padded = jnp.concatenate([fringe, gated_in], 1)
        conv_out = jnp.zeros_like(gated_in)
        for tap_index in range(reach + 1):
            conv_out = (
                conv_out + taps[layer_index, tap_index] * padded[:, tap_index : tap_index + rows]
            )
        branch = (out_gate * conv_out.reshape(parts * rows, wide)).astype(jnp.bfloat16)
        all_branch = lax.all_gather(branch, ("tp", "grp"), axis=1, tiled=True)
        acc_out = dot_by_blocks(all_branch, whole_out, here, slabs)
        mixed = lax.optimization_barrier(acc_out.astype(jnp.bfloat16))
        summed = residual_scale * hidden.astype(jnp.float32) + mixed.astype(jnp.float32)
        own_mean = jnp.mean(summed, axis=1)
        own_spread = jnp.mean(jnp.square(summed - own_mean[:, None]), axis=1)
        stats = lax.all_gather(jnp.stack([own_mean, own_spread]), ("tp", "grp"), axis=0)
        mean = jnp.mean(stats[:, 0], axis=0)
        variance = jnp.mean(stats[:, 1] + jnp.square(stats[:, 0] - mean), axis=0)[:, None]
        centered = summed - mean[:, None]
        hidden = (
            centered * lax.rsqrt(variance + norm_eps) * gain[layer_index] + bias[layer_index]
        ).astype(jnp.bfloat16)
    back = lax.all_to_all(
        hidden.reshape(parts, rows, out_wide), "grp", split_axis=0, concat_axis=1, tiled=False
    )
    return back.reshape(rows, parts * out_wide)


MESH = pl.DeviceIdType.MESH
BRANCH_CHUNKS = 5
SUM_CHUNKS = 5
BRANCH_AHEAD = 1
TOKEN_AHEAD = 1
TOKEN_HOOK = 2
SUM_AHEAD = 1
BRANCH_VIA_END = 1
SUM_VIA_END = 1
HALO = 32
VMEM_BYTES = 63 * 2**20


def multiple(value, of):
    return pl.multiple_of(value, of)


def tile_rows(rows, most):
    return max(n for n in range(16, most + 1, 16) if rows % n == 0)


def mixer_kernel(
    tokens, proj_b, proj_c, proj_x, proj_out, conv_taps, ln_gain, ln_bias, out,
    hidden, raw, branch, w_in, w_out, acc, carry, stage, final, scales, own_scales, stats, ones, means,
    local_sem, w_send, w_recv, ag_send, ag_recv, small_send, small_recv,
):
    f32, bf16 = jnp.float32, jnp.bfloat16
    residual_scale = (2.0 * LAYERS) ** 0.25
    g, s, t = (lax.axis_index(a) for a in ("grp", "sp", "tp"))
    parts, _, lanes = (lax.axis_size(a) for a in ("grp", "sp", "tp"))
    x, c = t // 2, t % 2
    rows, ow = tokens.shape
    kin, kout = proj_b.shape[1], proj_out.shape[1]
    wide, owide = proj_b.shape[2] // parts, ow // parts
    reach = conv_taps.shape[0] - 1
    part_rows = HALO + 2 * rows
    total = parts * part_rows
    half = s // 2
    base, end, mid = 2 * half, 3 * half, 1 + half
    other, far = 2 - half, 3 - 3 * half
    projections = (proj_b, proj_c, proj_x)
    kc = kin // 2
    pieces_in, pieces = (0, 1), 3

    def copy(src, dst, send, recv, device):
        return pltpu.make_async_remote_copy(src, dst, send, recv, device_id=device, device_id_type=MESH)

    def piece(layer, block, k):
        if k in pieces_in:
            return w_in.at[layer, pl.ds(multiple(block * kin + k * kc, kc), kc), :]
        return w_out.at[layer, pl.ds(multiple(block * kout, kout), kout), :]

    def piece_parts(layer, k):
        if k in pieces_in:
            columns = pl.ds(multiple(g * wide, wide), wide)
            rows_there = pl.ds(multiple(s * kin + k * kc, kc), kc)
            for j, w in enumerate(projections):
                yield w.at[layer, pl.ds(k * kc, kc), columns], w_in.at[layer, rows_there, pl.ds(j * wide, wide)]
        else:
            columns = pl.ds(multiple(g * owide, owide), owide)
            yield proj_out.at[layer, :, columns], piece(layer, s, k)

    def send_own(layer, k, device, row):
        sems = (w_send.at[row, layer * pieces + k], w_recv.at[row, layer * pieces + k])
        for src, dst in piece_parts(layer, k):
            copy(src, dst, *sems, device).start()

    def w_wait(layer, k, row, block, sent=False):
        ref = piece(layer, block, k)
        done = copy(ref, ref, w_send.at[row, layer * pieces + k], w_recv.at[row, layer * pieces + k], (g, s, t))
        done.wait_send() if sent else done.wait_recv()

    def relay(layer, k):
        w_wait(layer, k, 0, end)
        ref = piece(layer, end, k)
        sems = (w_send.at[2, layer * pieces + k], w_recv.at[2, layer * pieces + k])
        copy(ref, ref, *sems, (g, other, t)).start()

    order = [(layer, k) for layer in range(LAYERS) for k in range(pieces)]

    def token_rows(index):
        return pl.ds(multiple(g * part_rows + HALO + index * rows, 16), rows)

    def final_part(gg):
        return final.at[:, pl.ds(multiple(gg * owide, owide), owide)]

    def final_arrived(gg):
        ref = final_part(gg)
        copy(ref, ref, small_send.at[2], small_recv.at[8 + gg], (g, s, t)).wait_recv()

    yu, xu = g + c * (1 - 2 * g), x + (1 - c) * (1 - 2 * x)
    yv, xv = g + (1 - c) * (1 - 2 * g), x + c * (1 - 2 * x)
    up, vp, pp = (yu, s, 2 * xu + c), (yv, s, 2 * xv + c), (g, s, 2 * x + 1 - c)
    diagonal = (1 - g, s, 2 * (1 - x) + c)
    me = (g, s, t)

    def row_chunk(i, count):
        return pl.ds(multiple(i * (total // count), 16), total // count)

    def branch_columns(gg, tt):
        return pl.ds(multiple(tt * parts * wide + gg * wide, wide), wide)

    def branch_region(gg, tt, i):
        return row_chunk(i, BRANCH_CHUNKS), branch_columns(gg, tt)

    def sum_region(gg, tt, i):
        return row_chunk(i, SUM_CHUNKS), pl.ds(multiple(tt * ow + gg * owide, owide), owide)

    barrier = pltpu.get_barrier_semaphore()

    def greet(devices):
        for device in devices:
            pl.semaphore_signal(barrier, inc=1, device_id=device, device_id_type=MESH)
        pl.semaphore_wait(barrier, len(devices))

    lane_peers = [(g, s, (t + k) % lanes) for k in range(1, lanes)]

    def end_slab(j):
        start = multiple(g * part_rows + HALO + (end - base) * rows + j * (rows // 2), 16)
        return hidden.at[pl.ds(start, rows // 2), pl.ds(multiple(t * ow, ow), ow)]

    def end_tokens(j):
        return copy(
            tokens.at[pl.ds(j * (rows // 2), rows // 2), :], end_slab(j),
            small_send.at[3 * j], small_recv.at[3 * j], (g, mid, t),
        )

    @pl.when(s == end)
    def _():
        greet(lane_peers + [(1 - g, end, t)] + [(gg, mid, t) for gg in range(parts)])

        def send_tokens():
            for j in range(2):
                end_tokens(j).start()
            for j in range(2):
                end_tokens(j).wait_send()

        send_tokens()
        for layer, k in order:
            send_own(layer, k, (g, mid, t), 0)
            w_wait(layer, k, 0, s, sent=True)

        def pass_through(buffer, region, count, family, via):
            def transfer(owner, i, role, kind, device):
                ref = buffer.at[region(owner[0], owner[2], i)]
                return copy(ref, ref, ag_send.at[family, i, kind], ag_recv.at[family, i, role], device)

            through_end = range(count - via, count)
            for i in through_end:
                transfer(me, i, 3, 0, me).wait_recv()
                transfer(me, i, 0, 0, up).start()
                transfer(me, i, 1, 1, vp).start()
            for i in through_end:
                for role, owner in enumerate((up, vp, diagonal)):
                    transfer(me, i, role, 0, me).wait_recv()
                    if role == 0:
                        transfer(up, i, 2, 4, vp).start()
                    transfer(owner, i, role, (2, 3, 5)[role], (g, mid, t)).start()
            for i in through_end:
                for kind in range(6):
                    transfer(me, i, 0, kind, me).wait_send()

        pass_through(raw, sum_region, SUM_CHUNKS, 0, SUM_VIA_END)
        pass_through(branch, branch_region, BRANCH_CHUNKS, 2, BRANCH_VIA_END)
        for gg in range(parts):
            final_arrived(gg)

    @pl.when(s == mid)
    def _():
        there = (g, other, t)

        greet(lane_peers + [(1 - g, mid, t), there] + [(gg, end, t) for gg in range(parts)])
        for k in pieces_in:
            send_own(0, k, there, 1)
        mine = hidden.at[token_rows(mid - base), pl.ds(multiple(t * ow, ow), ow)]
        pltpu.make_async_copy(tokens, mine, local_sem.at[0]).start()
        for layer, k in order:
            for src, dst in piece_parts(layer, k):
                pltpu.make_async_copy(src, dst, local_sem.at[1 + layer * pieces + k]).start()

        edge = hidden.at[pl.ds(multiple(g * part_rows, 16), HALO), pl.ds(multiple(t * ow, ow), ow)]
        edge_copy = copy(tokens.at[pl.ds(rows - HALO, HALO), :], edge, small_send.at[1], small_recv.at[1], there)

        @pl.when(half == 0)
        def _():
            edge_copy.start()
            edge[...] = jnp.zeros_like(edge)

        own_scales[0:1, :] = ln_gain[0:1, :]
        own_scales[1:2, :] = ln_bias[0:1, :]
        scales[0:2, pl.ds(multiple(t * ow, ow), ow)] = own_scales[0:2, :]
        for k in range(1, lanes):
            copy(
                own_scales, scales.at[:, pl.ds(multiple(t * ow, ow), ow)],
                small_send.at[4 + k], small_recv.at[4 + k], (g, s, (t + k) % lanes),
            ).start()

        def gather(buffer, region, count, family, produce, consume, ahead, unroll=False, via=0, between=None):
            def at(device, i):
                return buffer.at[region(device[0], device[2], i)]

            def transfer(owner, i, role, kind, device):
                ref = at(owner, i)
                return copy(ref, ref, ag_send.at[family, i, kind], ag_recv.at[family, i, role], device)

            def arrived(i, role):
                transfer(me, i, role, 0, me).wait_recv()

            def send(i):
                produce(i)
                transfer(me, i, 0, 0, up).start()
                transfer(me, i, 1, 1, vp).start()
                transfer(me, i, 3, 2, pp).start()

            def pass_on(i):
                arrived(i, 0)
                transfer(up, i, 2, 4, vp).start()
                transfer(up, i, 4, 3, pp).start()
                arrived(i, 1)
                transfer(vp, i, 5, 5, pp).start()

            def finish(i):
                arrived(i, 2)
                transfer(diagonal, i, 6, 6, pp).start()
                for role in range(3, 7):
                    arrived(i, role)
                consume(i)

            def sent(i, kinds):
                for kind in kinds:
                    transfer(me, i, 0, kind, me).wait_send()

            through_end = range(count - via, count)
            for i in through_end:
                produce(i)
                transfer(me, i, 3, 0, (g, end, t)).start()
                transfer(me, i, 3, 2, pp).start()
            count = count - via
            for i in range(ahead):
                send(i)
            if unroll:
                for i in range(count + 1):
                    if i + ahead < count:
                        send(i + ahead)
                    if i < count:
                        pass_on(i)
                    if between:
                        between(i)
                    if i:
                        finish(i - 1)
            else:
                @pl.loop(0, count + 1)
                def _(i):
                    @pl.when(i + ahead < count)
                    def _():
                        send(i + ahead)

                    @pl.when(i < count)
                    def _():
                        pass_on(i)

                    @pl.when(i > 0)
                    def _():
                        finish(i - 1)

            for i in through_end:
                arrived(i, 0)
                transfer(up, i, 4, 3, pp).start()
                arrived(i, 1)
                transfer(vp, i, 5, 5, pp).start()
                finish(i)
                sent(i, (0, 2, 3, 5, 6))
            if unroll:
                for i in range(count):
                    sent(i, range(7))
            else:
                @pl.loop(0, count)
                def _(i):
                    sent(i, range(7))

        def nothing(i):
            pass

        first_half = rows // 2
        token_starts = (
            HALO + (mid - base) * rows,
            HALO + (mid - base) * rows + first_half,
            0,
            HALO + (end - base) * rows,
            HALO + (end - base) * rows + first_half,
        )

        def token_region(gg, tt, i):
            length = HALO if i == 2 else first_half
            return (
                pl.ds(multiple(gg * part_rows + token_starts[i], 16), length),
                pl.ds(multiple(tt * ow, ow), ow),
            )

        def token_ready(i):
            if i == 0:
                pltpu.make_async_copy(tokens, mine, local_sem.at[0]).wait()
            if i == 2:
                @pl.when(half == 1)
                def _():
                    edge_copy.wait_recv()
            if i > 2:
                slab = end_slab(i - 3)
                copy(slab, slab, small_send.at[3 * (i - 3)], small_recv.at[3 * (i - 3)], me).wait_recv()

        def token_hook(i):
            if i == TOKEN_HOOK:
                relay(0, 0)
            if i == 4:
                relay(0, 1)

        gather(hidden, token_region, 5, 0, token_ready, nothing, TOKEN_AHEAD, unroll=True, between=token_hook)

        def accumulate(layer, start, depth, at_rows, first=False):
            term = jnp.dot(
                hidden[at_rows, pl.ds(multiple(start, kc), depth)],
                w_in[layer, pl.ds(multiple(start, kc), depth), :],
                preferred_element_type=f32,
            )
            acc[at_rows, :] = term if first else acc[at_rows, :] + term

        def wait_near(layer, k):
            ref = piece(layer, s, k)
            pltpu.make_async_copy(ref, ref, local_sem.at[1 + layer * pieces + k]).wait()

        def near_in(layer, at_rows):
            accumulate(layer, base * kin, 2 * kin, at_rows, first=True)

        def far_in(layer):
            def add(start, depth):
                @pl.loop(0, 4)
                def _(i):
                    accumulate(layer, start, depth, row_chunk(i, 4))

            for k in pieces_in:
                w_wait(layer, k, 1, other)
            add(other * kin, kin)
            for k in pieces_in:
                w_wait(layer, k, 2, far)
                add(far * kin + k * kc, kc)

        tr = tile_rows(total // 10, 96)

        def gate(layer, i):
            taps = [
                conv_taps[n, layer : layer + 1, pl.ds(multiple(g * wide, wide), wide)] for n in range(reach + 1)
            ]
            row_of = lax.broadcasted_iota(jnp.int32, (tr, wide), 0)
            first = i * (total // BRANCH_CHUNKS)
            sums = acc[pl.ds(multiple(jnp.maximum(first - 8, 0), 8), 8), wide:].astype(bf16).astype(f32)
            unseen = HALO * (1 - half) - (first - 8) % part_rows
            carry[...] = jnp.where(row_of[:8] < unseen, 0.0, sums[:, :wide] * sums[:, wide:])

            @pl.loop(0, total // BRANCH_CHUNKS // tr)
            def _(q):
                start = multiple(i * (total // BRANCH_CHUNKS) + q * tr, 16)
                position = start % part_rows
                sums = acc[pl.ds(start, tr), :].astype(bf16).astype(f32)
                out_gate, in_gate, values = (sums[:, j * wide : (j + 1) * wide] for j in range(3))
                gated = in_gate * values
                gated = jnp.where(row_of < HALO * (1 - half) - position, 0.0, gated)
                before = jnp.where(position == 0, 0.0, carry[...])
                conv = jnp.zeros_like(gated)
                for n in range(reach + 1):
                    shift = reach - n
                    moved = gated
                    if shift:
                        moved = pltpu.roll(gated, shift, 0)
                        for j in range(shift):
                            moved = jnp.where(row_of == j, before[8 - shift + j : 8 - shift + j + 1, :], moved)
                    conv = conv + taps[n] * moved
                carry[...] = gated[tr - 8 :, :]
                branch[pl.ds(start, tr), branch_columns(g, t)] = (out_gate * conv).astype(bf16)

        def wait_out(layer):
            wait_near(layer, 2)
            for row, block in ((1, other), (2, far)):
                w_wait(layer, 2, row, block)

        own_columns = pl.ds(multiple(t * ow + g * owide, owide), owide)

        def mix(layer, at_rows):
            mixed = jnp.dot(branch[at_rows, :], w_out[layer], preferred_element_type=f32)
            kept = hidden[at_rows, own_columns].astype(f32)
            return (residual_scale * kept + mixed.astype(bf16).astype(f32)).astype(bf16)

        def produce_sum(i):
            at_rows = row_chunk(i, SUM_CHUNKS)
            raw[at_rows, own_columns] = mix(0, at_rows)

        strips = [slice(n, n + 128) for n in range(0, hidden.shape[1], 128)]
        ones[...] = jnp.ones_like(ones)

        def normalise(i):
            means[...] = jnp.dot(raw[row_chunk(i, SUM_CHUNKS), :], ones[...], preferred_element_type=f32) / ones.shape[0]

            @pl.loop(0, total // SUM_CHUNKS // tr)
            def _(q):
                there_rows = pl.ds(multiple(i * (total // SUM_CHUNKS) + q * tr, 16), tr)
                here_rows = pl.ds(multiple(q * tr, 16), tr)
                mean = means[here_rows, :]
                squares = jnp.zeros_like(mean)
                for strip in strips:
                    centered = raw[there_rows, strip].astype(f32) - mean
                    squares = squares + centered * centered
                scale = lax.rsqrt(jnp.sum(squares, axis=1, keepdims=True) / ones.shape[0] + norm_eps)
                scale = jnp.broadcast_to(scale, mean.shape)
                for strip in strips:
                    centered = raw[there_rows, strip].astype(f32) - mean
                    hidden[there_rows, strip] = (
                        centered * scale * scales[0:1, strip] + scales[1:2, strip]
                    ).astype(bf16)

        def send_pair(layer, k):
            send_own(layer, k, there, 1)
            relay(layer, k)

        def consume_sum(i):
            normalise(i)
            near_in(1, row_chunk(i, SUM_CHUNKS))

            @pl.when(i == 2)
            def _():
                send_pair(1, 2)

        def first_branches(i):
            @pl.when(i == BRANCH_CHUNKS - 2)
            def _():
                send_pair(1, 0)

        for k in pieces_in:
            wait_near(0, k)

        @pl.loop(0, 4)
        def _(i):
            near_in(0, row_chunk(i, 4))

        far_in(0)
        send_pair(0, 2)
        gather(
            branch, branch_region, BRANCH_CHUNKS, 1, lambda i: gate(0, i), first_branches, BRANCH_AHEAD
        )
        send_pair(1, 1)
        for k in range(1, lanes):
            copy(
                own_scales, scales.at[:, pl.ds(multiple(((t + lanes - k) % lanes) * ow, ow), ow)],
                small_send.at[4 + k], small_recv.at[4 + k], me,
            ).wait()
        wait_out(0)
        for k in pieces_in:
            wait_near(1, k)
        gather(raw, sum_region, SUM_CHUNKS, 0, produce_sum, consume_sum, SUM_AHEAD, via=SUM_VIA_END)
        far_in(1)
        gather(
            branch, branch_region, BRANCH_CHUNKS, 2, lambda i: gate(1, i), nothing, BRANCH_AHEAD,
            via=BRANCH_VIA_END,
        )
        wait_out(1)

        def result_copy(j):
            p = (g + 1 + j // 2) % 2
            to = end + (j % 2) * (mid - end)
            return p, to, copy(
                stage.at[j], final_part(g), small_send.at[12 + j], small_recv.at[8 + g], (p, to, t)
            )

        @pl.loop(0, 4)
        def _(j):
            p, to, result = result_copy(j)
            stage[j] = mix(1, pl.ds(multiple(p * part_rows + HALO + (to - base) * rows, 16), rows))

            @pl.when(j < 3)
            def _():
                result.start()

        final[:, pl.ds(multiple(g * owide, owide), owide)] = stage[3]
        for j in range(3):
            result_copy(j)[2].wait_send()
        for layer, k in order:
            w_wait(layer, k, 1, s, sent=True)
            w_wait(layer, k, 2, end, sent=True)

        @pl.when(half == 0)
        def _():
            edge_copy.wait_send()

        final_arrived(1 - g)

    lane = lax.broadcasted_iota(jnp.int32, (128, 128), 1)
    line = lax.broadcasted_iota(jnp.int32, (128, 128), 0)

    @pl.loop(0, rows // 128)
    def _(b):
        at_rows = pl.ds(multiple(b * 128, 128), 128)
        summed = final[at_rows, :].astype(f32)
        mean = jnp.mean(summed, axis=1, keepdims=True)
        spread = jnp.mean(jnp.square(summed - mean), axis=1, keepdims=True)
        packed = jnp.where(lane == 0, mean, jnp.where(lane == 1, spread, 0.0))
        stats[t, :, at_rows] = packed.T[0:8, :]

    def stat_copy(k, owner):
        return copy(
            stats.at[owner], stats.at[owner], small_send.at[4 + k], small_recv.at[16 + k], (g, s, (t + k) % lanes)
        )

    for k in range(1, lanes):
        stat_copy(k, t).start()
    for k in range(1, lanes):
        stat_copy(k, (t + lanes - k) % lanes).wait()

    @pl.loop(0, rows // 128)
    def _(b):
        at_rows = pl.ds(multiple(b * 128, 128), 128)
        means = [stats[i, 0:1, at_rows] for i in range(lanes)]
        mean = sum(means) / lanes
        variance = sum(stats[i, 1:2, at_rows] + jnp.square(means[i] - mean) for i in range(lanes)) / lanes
        packed = jnp.where(line == 0, mean, jnp.where(line == 1, lax.rsqrt(variance + norm_eps), 0.0)).T
        centered = final[at_rows, :].astype(f32) - packed[:, 0:1]
        out[at_rows, :] = (
            centered * packed[:, 1:2] * ln_gain[LAYERS - 1 : LAYERS, :] + ln_bias[LAYERS - 1 : LAYERS, :]
        ).astype(bf16)


def mixer(tokens, proj_b, proj_c, proj_x, proj_out, conv_taps, ln_gain, ln_bias):
    parts, slabs, lanes = (lax.axis_size(a) for a in ("grp", "sp", "tp"))
    f32, bf16 = jnp.float32, jnp.bfloat16
    rows, ow = tokens.shape
    depth, channels = slabs * proj_b.shape[1], slabs * proj_out.shape[1]
    wide, owide = proj_b.shape[2] // parts, ow // parts
    total = parts * (HALO + 2 * rows)
    dma = pltpu.SemaphoreType.DMA
    anywhere, vmem = pl.BlockSpec(memory_space=pl.ANY), pl.BlockSpec(memory_space=pltpu.VMEM)
    return pl.pallas_call(
        mixer_kernel,
        out_shape=jax.ShapeDtypeStruct((rows, ow), bf16),
        in_specs=[anywhere] * 5 + [vmem] * 3,
        out_specs=vmem,
        scratch_shapes=[
            pltpu.VMEM((total, depth), bf16),
            pltpu.VMEM((total, depth), bf16),
            pltpu.VMEM((total, channels), bf16),
            pltpu.VMEM((LAYERS, depth, 3 * wide), bf16),
            pltpu.VMEM((LAYERS, channels, owide), bf16),
            pltpu.VMEM((total, 3 * wide), f32),
            pltpu.VMEM((8, wide), f32),
            pltpu.VMEM((4, rows, owide), bf16),
            pltpu.VMEM((rows, ow), bf16),
            pltpu.VMEM((8, depth), f32),
            pltpu.VMEM((8, ow), f32),
            pltpu.VMEM((lanes, 8, rows), f32),
            pltpu.VMEM((depth, 128), bf16),
            pltpu.VMEM((total // SUM_CHUNKS, 128), f32),
            dma((1 + 3 * LAYERS,)),
            dma((3, 3 * LAYERS)),
            dma((3, 3 * LAYERS)),
            dma((3, max(5, SUM_CHUNKS, BRANCH_CHUNKS), 7)),
            dma((3, max(5, SUM_CHUNKS, BRANCH_CHUNKS), 7)),
            dma((20,)),
            dma((20,)),
        ],
        compiler_params=pltpu.CompilerParams(
            has_side_effects=True, collective_id=0, vmem_limit_bytes=VMEM_BYTES
        ),
    )(tokens, proj_b, proj_c, proj_x, proj_out, conv_taps.transpose(1, 0, 2), ln_gain, ln_bias)


def solution(mesh):
    specs = dict(
        mesh=mesh,
        in_specs=(
            P(("grp", "sp"), "tp"),
            P(None, "sp", "tp"),
            P(None, "sp", "tp"),
            P(None, "sp", "tp"),
            P(None, "sp", "tp"),
            P(None, None, "tp"),
            P(None, "tp"),
            P(None, "tp"),
        ),
        out_specs=P(("grp", "sp"), "tp"),
        check_vma=False,
    )
    if (mesh.shape["grp"], mesh.shape["sp"], mesh.shape["tp"]) == (2, 4, 4):
        return jax.shard_map(mixer, **specs)
    return jax.shard_map(local, **specs)
```

```python
import jax
import jax.numpy as jnp
from jax import lax
from jax.experimental import pallas as pl
from jax.experimental.pallas import tpu as pltpu
from jax.sharding import PartitionSpec as P


LAYERS = 2


norm_eps = 1e-05


def from_behind(block, axis, distance):
    devices = range(lax.axis_size(axis))
    route = [(i - distance, i) for i in devices if i - distance in devices]
    return lax.ppermute(block, axis, route)


def along_line(block, axis, earlier):
    size = lax.axis_size(axis)
    blocks, latest = [(0, block)], []
    for side, step in enumerate((1, -1)):
        moving = block
        if earlier:
            moving, _ = lax.optimization_barrier((moving, earlier[side]))
        hops = []
        for hop in range(1, size):
            start = range(hop - 1, size - 1) if step == 1 else range(1, size - hop + 1)
            moving = lax.ppermute(moving, axis, [(i, i + step) for i in start])
            hops.append((-step * hop, moving))
        latest.append(hops[max(len(hops) - 2, 0)][1])
        blocks += hops
    return sorted(blocks, key=lambda b: abs(b[0])), latest


def dot_by_blocks(left, blocks, here, size):
    total = None
    for offset, block in blocks:
        depth = block.shape[0]
        owner = jnp.clip(here + offset, 0, size - 1)
        columns = lax.dynamic_slice_in_dim(left, owner * depth, depth, 1)
        term = jnp.dot(columns, block, preferred_element_type=jnp.float32)
        total = term if total is None else total + term
    return total


def local(tokens, proj_b, proj_c, proj_x, proj_out, conv_taps, ln_gain, ln_bias):
    residual_scale = (2.0 * LAYERS) ** 0.25
    parts = lax.axis_size("grp")
    me = lax.axis_index("grp")
    rows = tokens.shape[0]
    wide = proj_b.shape[2] // parts
    out_wide = proj_out.shape[2] // parts

    def mine(array, width):
        return lax.dynamic_slice_in_dim(array, me * width, width, array.ndim - 1)

    slabs, here = lax.axis_size("sp"), lax.axis_index("sp")
    weights = []
    earlier = None
    for layer_index in range(LAYERS):
        ins = jnp.concatenate(
            [mine(w[layer_index], wide) for w in (proj_b, proj_c, proj_x)], axis=1
        )
        ins, earlier = along_line(ins, "sp", earlier)
        outs, earlier = along_line(mine(proj_out[layer_index], out_wide), "sp", earlier)
        weights.append((ins, outs))
    taps, gain, bias = mine(conv_taps, wide), mine(ln_gain, out_wide), mine(ln_bias, out_wide)
    swapped = lax.all_to_all(
        tokens.reshape(rows, parts, out_wide), "grp", split_axis=1, concat_axis=0, tiled=False
    )
    hidden = swapped.reshape(parts * rows, out_wide)
    reach = taps.shape[1] - 1
    for layer_index in range(LAYERS):
        whole_in, whole_out = weights[layer_index]
        gathered = lax.all_gather(hidden, ("tp", "grp"), axis=1, tiled=True)
        acc = dot_by_blocks(gathered, whole_in, here, slabs)
        acc = lax.optimization_barrier(acc.astype(jnp.bfloat16)).astype(jnp.float32)
        out_gate, in_gate, values = (acc[:, i * wide : (i + 1) * wide] for i in range(3))
        gated_in = (in_gate * values).reshape(parts, rows, wide)
        fringe = from_behind(gated_in[:, rows - reach :], "sp", 1)
        padded = jnp.concatenate([fringe, gated_in], 1)
        conv_out = jnp.zeros_like(gated_in)
        for tap_index in range(reach + 1):
            conv_out = (
                conv_out + taps[layer_index, tap_index] * padded[:, tap_index : tap_index + rows]
            )
        branch = (out_gate * conv_out.reshape(parts * rows, wide)).astype(jnp.bfloat16)
        all_branch = lax.all_gather(branch, ("tp", "grp"), axis=1, tiled=True)
        acc_out = dot_by_blocks(all_branch, whole_out, here, slabs)
        mixed = lax.optimization_barrier(acc_out.astype(jnp.bfloat16))
        summed = residual_scale * hidden.astype(jnp.float32) + mixed.astype(jnp.float32)
        own_mean = jnp.mean(summed, axis=1)
        own_spread = jnp.mean(jnp.square(summed - own_mean[:, None]), axis=1)
        stats = lax.all_gather(jnp.stack([own_mean, own_spread]), ("tp", "grp"), axis=0)
        mean = jnp.mean(stats[:, 0], axis=0)
        variance = jnp.mean(stats[:, 1] + jnp.square(stats[:, 0] - mean), axis=0)[:, None]
        centered = summed - mean[:, None]
        hidden = (
            centered * lax.rsqrt(variance + norm_eps) * gain[layer_index] + bias[layer_index]
        ).astype(jnp.bfloat16)
    back = lax.all_to_all(
        hidden.reshape(parts, rows, out_wide), "grp", split_axis=0, concat_axis=1, tiled=False
    )
    return back.reshape(rows, parts * out_wide)


MESH = pl.DeviceIdType.MESH
BRANCH_CHUNKS = 5
SUM_CHUNKS = 5
BRANCH_AHEAD = 1
TOKEN_AHEAD = 1
OWN_HOOK = 2
OUT_EARLY = False
OUT_HOOK = 2
NEXT_HOOK = 2
SUM_AHEAD = 1
BRANCH_VIA_END = 1
SUM_VIA_END = 1
HALO = 32
VMEM_BYTES = 63 * 2**20


def multiple(value, of):
    return pl.multiple_of(value, of)


def tile_rows(rows, most):
    return max(n for n in range(16, most + 1, 16) if rows % n == 0)


def mixer_kernel(
    tokens, proj_b, proj_c, proj_x, proj_out, conv_taps, ln_gain, ln_bias, out,
    hidden, raw, branch, w_in, w_out, acc, carry, stage, final, scales, own_scales, stats, ones, means,
    local_sem, w_send, w_recv, ag_send, ag_recv, small_send, small_recv,
):
    f32, bf16 = jnp.float32, jnp.bfloat16
    residual_scale = (2.0 * LAYERS) ** 0.25
    g, s, t = (lax.axis_index(a) for a in ("grp", "sp", "tp"))
    parts, _, lanes = (lax.axis_size(a) for a in ("grp", "sp", "tp"))
    x, c = t // 2, t % 2
    rows, ow = tokens.shape
    kin, kout = proj_b.shape[1], proj_out.shape[1]
    wide, owide = proj_b.shape[2] // parts, ow // parts
    reach = conv_taps.shape[0] - 1
    part_rows = HALO + 2 * rows
    total = parts * part_rows
    half = s // 2
    base, end, mid = 2 * half, 3 * half, 1 + half
    other, far = 2 - half, 3 - 3 * half
    projections = (proj_b, proj_c, proj_x)
    kc = kin // 2
    pieces_in, pieces = (0, 1), 3

    def copy(src, dst, send, recv, device):
        return pltpu.make_async_remote_copy(src, dst, send, recv, device_id=device, device_id_type=MESH)

    def piece(layer, block, k):
        if k in pieces_in:
            return w_in.at[layer, pl.ds(multiple(block * kin + k * kc, kc), kc), :]
        return w_out.at[layer, pl.ds(multiple(block * kout, kout), kout), :]

    def piece_parts(layer, k):
        if k in pieces_in:
            columns = pl.ds(multiple(g * wide, wide), wide)
            rows_there = pl.ds(multiple(s * kin + k * kc, kc), kc)
            for j, w in enumerate(projections):
                yield w.at[layer, pl.ds(k * kc, kc), columns], w_in.at[layer, rows_there, pl.ds(j * wide, wide)]
        else:
            columns = pl.ds(multiple(g * owide, owide), owide)
            yield proj_out.at[layer, :, columns], piece(layer, s, k)

    def send_own(layer, k, device, row):
        sems = (w_send.at[row, layer * pieces + k], w_recv.at[row, layer * pieces + k])
        for src, dst in piece_parts(layer, k):
            copy(src, dst, *sems, device).start()

    def w_wait(layer, k, row, block, sent=False):
        ref = piece(layer, block, k)
        done = copy(ref, ref, w_send.at[row, layer * pieces + k], w_recv.at[row, layer * pieces + k], (g, s, t))
        done.wait_send() if sent else done.wait_recv()

    def relay(layer, k):
        w_wait(layer, k, 0, end)
        ref = piece(layer, end, k)
        sems = (w_send.at[2, layer * pieces + k], w_recv.at[2, layer * pieces + k])
        copy(ref, ref, *sems, (g, other, t)).start()

    order = [(layer, k) for layer in range(LAYERS) for k in range(pieces)]

    def token_rows(index):
        return pl.ds(multiple(g * part_rows + HALO + index * rows, 16), rows)

    def final_part(gg):
        return final.at[:, pl.ds(multiple(gg * owide, owide), owide)]

    def final_arrived(gg):
        ref = final_part(gg)
        copy(ref, ref, small_send.at[2], small_recv.at[8 + gg], (g, s, t)).wait_recv()

    yu, xu = g + c * (1 - 2 * g), x + (1 - c) * (1 - 2 * x)
    yv, xv = g + (1 - c) * (1 - 2 * g), x + c * (1 - 2 * x)
    up, vp, pp = (yu, s, 2 * xu + c), (yv, s, 2 * xv + c), (g, s, 2 * x + 1 - c)
    diagonal = (1 - g, s, 2 * (1 - x) + c)
    me = (g, s, t)

    def row_chunk(i, count):
        return pl.ds(multiple(i * (total // count), 16), total // count)

    def branch_columns(gg, tt):
        return pl.ds(multiple(tt * parts * wide + gg * wide, wide), wide)

    def branch_region(gg, tt, i):
        return row_chunk(i, BRANCH_CHUNKS), branch_columns(gg, tt)

    def sum_region(gg, tt, i):
        return row_chunk(i, SUM_CHUNKS), pl.ds(multiple(tt * ow + gg * owide, owide), owide)

    barrier = pltpu.get_barrier_semaphore()

    def greet(devices):
        for device in devices:
            pl.semaphore_signal(barrier, inc=1, device_id=device, device_id_type=MESH)
        pl.semaphore_wait(barrier, len(devices))

    lane_peers = [(g, s, (t + k) % lanes) for k in range(1, lanes)]

    def end_slab(j):
        start = multiple(g * part_rows + HALO + (end - base) * rows + j * (rows // 2), 16)
        return hidden.at[pl.ds(start, rows // 2), pl.ds(multiple(t * ow, ow), ow)]

    def end_tokens(j):
        return copy(
            tokens.at[pl.ds(j * (rows // 2), rows // 2), :], end_slab(j),
            small_send.at[3 * j], small_recv.at[3 * j], (g, mid, t),
        )

    @pl.when(s == end)
    def _():
        greet(lane_peers + [(1 - g, end, t)] + [(gg, mid, t) for gg in range(parts)])

        def send_tokens():
            for j in range(2):
                end_tokens(j).start()
            for j in range(2):
                end_tokens(j).wait_send()

        for layer, k in order:
            send_own(layer, k, (g, mid, t), 0)
            w_wait(layer, k, 0, s, sent=True)
            if (layer, k) == (0, 0):
                send_tokens()

        def pass_through(buffer, region, count, family, via):
            def transfer(owner, i, role, kind, device):
                ref = buffer.at[region(owner[0], owner[2], i)]
                return copy(ref, ref, ag_send.at[family, i, kind], ag_recv.at[family, i, role], device)

            through_end = range(count - via, count)
            for i in through_end:
                transfer(me, i, 3, 0, me).wait_recv()
                transfer(me, i, 0, 0, up).start()
                transfer(me, i, 1, 1, vp).start()
            for i in through_end:
                for role, owner in enumerate((up, vp, diagonal)):
                    transfer(me, i, role, 0, me).wait_recv()
                    if role == 0:
                        transfer(up, i, 2, 4, vp).start()
                    transfer(owner, i, role, (2, 3, 5)[role], (g, mid, t)).start()
            for i in through_end:
                for kind in range(6):
                    transfer(me, i, 0, kind, me).wait_send()

        pass_through(raw, sum_region, SUM_CHUNKS, 0, SUM_VIA_END)
        pass_through(branch, branch_region, BRANCH_CHUNKS, 2, BRANCH_VIA_END)
        for gg in range(parts):
            final_arrived(gg)

    @pl.when(s == mid)
    def _():
        there = (g, other, t)

        greet(lane_peers + [(1 - g, mid, t), there] + [(gg, end, t) for gg in range(parts)])
        send_own(0, 0, there, 1)
        mine = hidden.at[token_rows(mid - base), pl.ds(multiple(t * ow, ow), ow)]
        pltpu.make_async_copy(tokens, mine, local_sem.at[0]).start()
        for layer, k in order:
            for src, dst in piece_parts(layer, k):
                pltpu.make_async_copy(src, dst, local_sem.at[1 + layer * pieces + k]).start()

        edge = hidden.at[pl.ds(multiple(g * part_rows, 16), HALO), pl.ds(multiple(t * ow, ow), ow)]
        edge_copy = copy(tokens.at[pl.ds(rows - HALO, HALO), :], edge, small_send.at[1], small_recv.at[1], there)

        @pl.when(half == 0)
        def _():
            edge_copy.start()
            edge[...] = jnp.zeros_like(edge)

        own_scales[0:1, :] = ln_gain[0:1, :]
        own_scales[1:2, :] = ln_bias[0:1, :]
        scales[0:2, pl.ds(multiple(t * ow, ow), ow)] = own_scales[0:2, :]
        for k in range(1, lanes):
            copy(
                own_scales, scales.at[:, pl.ds(multiple(t * ow, ow), ow)],
                small_send.at[4 + k], small_recv.at[4 + k], (g, s, (t + k) % lanes),
            ).start()

        def gather(buffer, region, count, family, produce, consume, ahead, unroll=False, via=0, between=None):
            def at(device, i):
                return buffer.at[region(device[0], device[2], i)]

            def transfer(owner, i, role, kind, device):
                ref = at(owner, i)
                return copy(ref, ref, ag_send.at[family, i, kind], ag_recv.at[family, i, role], device)

            def arrived(i, role):
                transfer(me, i, role, 0, me).wait_recv()

            def send(i):
                produce(i)
                transfer(me, i, 0, 0, up).start()
                transfer(me, i, 1, 1, vp).start()
                transfer(me, i, 3, 2, pp).start()

            def pass_on(i):
                arrived(i, 0)
                transfer(up, i, 2, 4, vp).start()
                transfer(up, i, 4, 3, pp).start()
                arrived(i, 1)
                transfer(vp, i, 5, 5, pp).start()

            def finish(i):
                arrived(i, 2)
                transfer(diagonal, i, 6, 6, pp).start()
                for role in range(3, 7):
                    arrived(i, role)
                consume(i)

            def sent(i, kinds):
                for kind in kinds:
                    transfer(me, i, 0, kind, me).wait_send()

            through_end = range(count - via, count)
            for i in through_end:
                produce(i)
                transfer(me, i, 3, 0, (g, end, t)).start()
                transfer(me, i, 3, 2, pp).start()
            count = count - via
            for i in range(ahead):
                send(i)
            if unroll:
                for i in range(count + 1):
                    if i + ahead < count:
                        send(i + ahead)
                    if i < count:
                        pass_on(i)
                    if between:
                        between(i)
                    if i:
                        finish(i - 1)
            else:
                @pl.loop(0, count + 1)
                def _(i):
                    @pl.when(i + ahead < count)
                    def _():
                        send(i + ahead)

                    @pl.when(i < count)
                    def _():
                        pass_on(i)

                    @pl.when(i > 0)
                    def _():
                        finish(i - 1)

            for i in through_end:
                arrived(i, 0)
                transfer(up, i, 4, 3, pp).start()
                arrived(i, 1)
                transfer(vp, i, 5, 5, pp).start()
                finish(i)
                sent(i, (0, 2, 3, 5, 6))
            if unroll:
                for i in range(count):
                    sent(i, range(7))
            else:
                @pl.loop(0, count)
                def _(i):
                    sent(i, range(7))

        def nothing(i):
            pass

        first_half = rows // 2
        token_starts = (
            HALO + (mid - base) * rows,
            HALO + (mid - base) * rows + first_half,
            0,
            HALO + (end - base) * rows,
            HALO + (end - base) * rows + first_half,
        )

        def token_region(gg, tt, i):
            length = HALO if i == 2 else first_half
            return (
                pl.ds(multiple(gg * part_rows + token_starts[i], 16), length),
                pl.ds(multiple(tt * ow, ow), ow),
            )

        def token_ready(i):
            if i == 0:
                pltpu.make_async_copy(tokens, mine, local_sem.at[0]).wait()
            if i == 2:
                @pl.when(half == 1)
                def _():
                    edge_copy.wait_recv()
            if i > 2:
                slab = end_slab(i - 3)
                copy(slab, slab, small_send.at[3 * (i - 3)], small_recv.at[3 * (i - 3)], me).wait_recv()

        def token_hook(i):
            if i == 1:
                relay(0, 0)
            if i == OWN_HOOK:
                send_own(0, 1, there, 1)
            if i == 4:
                relay(0, 1)

        gather(hidden, token_region, 5, 0, token_ready, nothing, TOKEN_AHEAD, unroll=True, between=token_hook)

        def accumulate(layer, start, depth, at_rows, first=False):
            term = jnp.dot(
                hidden[at_rows, pl.ds(multiple(start, kc), depth)],
                w_in[layer, pl.ds(multiple(start, kc), depth), :],
                preferred_element_type=f32,
            )
            acc[at_rows, :] = term if first else acc[at_rows, :] + term

        def wait_near(layer, k):
            ref = piece(layer, s, k)
            pltpu.make_async_copy(ref, ref, local_sem.at[1 + layer * pieces + k]).wait()

        def near_in(layer, at_rows):
            accumulate(layer, base * kin, 2 * kin, at_rows, first=True)

        def far_in(layer):
            def add(start, depth):
                @pl.loop(0, 4)
                def _(i):
                    accumulate(layer, start, depth, row_chunk(i, 4))

            for k in pieces_in:
                w_wait(layer, k, 1, other)
            add(other * kin, kin)
            for k in pieces_in:
                w_wait(layer, k, 2, far)
                add(far * kin + k * kc, kc)

        tr = tile_rows(total // 10, 96)

        def gate(layer, i):
            taps = [
                conv_taps[n, layer : layer + 1, pl.ds(multiple(g * wide, wide), wide)] for n in range(reach + 1)
            ]
            row_of = lax.broadcasted_iota(jnp.int32, (tr, wide), 0)
            first = i * (total // BRANCH_CHUNKS)
            sums = acc[pl.ds(multiple(jnp.maximum(first - 8, 0), 8), 8), wide:].astype(bf16).astype(f32)
            unseen = HALO * (1 - half) - (first - 8) % part_rows
            carry[...] = jnp.where(row_of[:8] < unseen, 0.0, sums[:, :wide] * sums[:, wide:])

            @pl.loop(0, total // BRANCH_CHUNKS // tr)
            def _(q):
                start = multiple(i * (total // BRANCH_CHUNKS) + q * tr, 16)
                position = start % part_rows
                sums = acc[pl.ds(start, tr), :].astype(bf16).astype(f32)
                out_gate, in_gate, values = (sums[:, j * wide : (j + 1) * wide] for j in range(3))
                gated = in_gate * values
                gated = jnp.where(row_of < HALO * (1 - half) - position, 0.0, gated)
                before = jnp.where(position == 0, 0.0, carry[...])
                conv = jnp.zeros_like(gated)
                for n in range(reach + 1):
                    shift = reach - n
                    moved = gated
                    if shift:
                        moved = pltpu.roll(gated, shift, 0)
                        for j in range(shift):
                            moved = jnp.where(row_of == j, before[8 - shift + j : 8 - shift + j + 1, :], moved)
                    conv = conv + taps[n] * moved
                carry[...] = gated[tr - 8 :, :]
                branch[pl.ds(start, tr), branch_columns(g, t)] = (out_gate * conv).astype(bf16)

        def wait_out(layer):
            wait_near(layer, 2)
            for row, block in ((1, other), (2, far)):
                w_wait(layer, 2, row, block)

        own_columns = pl.ds(multiple(t * ow + g * owide, owide), owide)

        def mix(layer, at_rows):
            mixed = jnp.dot(branch[at_rows, :], w_out[layer], preferred_element_type=f32)
            kept = hidden[at_rows, own_columns].astype(f32)
            return (residual_scale * kept + mixed.astype(bf16).astype(f32)).astype(bf16)

        def produce_sum(i):
            at_rows = row_chunk(i, SUM_CHUNKS)
            raw[at_rows, own_columns] = mix(0, at_rows)

        strips = [slice(n, n + 128) for n in range(0, hidden.shape[1], 128)]
        ones[...] = jnp.ones_like(ones)

        def normalise(i):
            means[...] = jnp.dot(raw[row_chunk(i, SUM_CHUNKS), :], ones[...], preferred_element_type=f32) / ones.shape[0]

            @pl.loop(0, total // SUM_CHUNKS // tr)
            def _(q):
                there_rows = pl.ds(multiple(i * (total // SUM_CHUNKS) + q * tr, 16), tr)
                here_rows = pl.ds(multiple(q * tr, 16), tr)
                mean = means[here_rows, :]
                squares = jnp.zeros_like(mean)
                for strip in strips:
                    centered = raw[there_rows, strip].astype(f32) - mean
                    squares = squares + centered * centered
                scale = lax.rsqrt(jnp.sum(squares, axis=1, keepdims=True) / ones.shape[0] + norm_eps)
                scale = jnp.broadcast_to(scale, mean.shape)
                for strip in strips:
                    centered = raw[there_rows, strip].astype(f32) - mean
                    hidden[there_rows, strip] = (
                        centered * scale * scales[0:1, strip] + scales[1:2, strip]
                    ).astype(bf16)

        def send_pair(layer, k):
            send_own(layer, k, there, 1)
            relay(layer, k)

        def consume_sum(i):
            normalise(i)
            near_in(1, row_chunk(i, SUM_CHUNKS))

            @pl.when(i == OUT_HOOK)
            def _():
                send_pair(1, 2)

        def first_branches(i):
            @pl.when(i == BRANCH_CHUNKS - NEXT_HOOK)
            def _():
                send_pair(1, 0)

        for k in pieces_in:
            wait_near(0, k)

        @pl.loop(0, 4)
        def _(i):
            near_in(0, row_chunk(i, 4))

        if OUT_EARLY:
            send_pair(0, 2)
        far_in(0)
        if not OUT_EARLY:
            send_pair(0, 2)
        gather(
            branch, branch_region, BRANCH_CHUNKS, 1, lambda i: gate(0, i), first_branches, BRANCH_AHEAD
        )
        send_pair(1, 1)
        for k in range(1, lanes):
            copy(
                own_scales, scales.at[:, pl.ds(multiple(((t + lanes - k) % lanes) * ow, ow), ow)],
                small_send.at[4 + k], small_recv.at[4 + k], me,
            ).wait()
        wait_out(0)
        for k in pieces_in:
            wait_near(1, k)
        gather(raw, sum_region, SUM_CHUNKS, 0, produce_sum, consume_sum, SUM_AHEAD, via=SUM_VIA_END)
        far_in(1)
        gather(
            branch, branch_region, BRANCH_CHUNKS, 2, lambda i: gate(1, i), nothing, BRANCH_AHEAD,
            via=BRANCH_VIA_END,
        )
        wait_out(1)

        def result_copy(j):
            p = (g + 1 + j // 2) % 2
            to = end + (j % 2) * (mid - end)
            return p, to, copy(
                stage.at[j], final_part(g), small_send.at[12 + j], small_recv.at[8 + g], (p, to, t)
            )

        @pl.loop(0, 4)
        def _(j):
            p, to, result = result_copy(j)
            stage[j] = mix(1, pl.ds(multiple(p * part_rows + HALO + (to - base) * rows, 16), rows))

            @pl.when(j < 3)
            def _():
                result.start()

        final[:, pl.ds(multiple(g * owide, owide), owide)] = stage[3]
        for j in range(3):
            result_copy(j)[2].wait_send()
        for layer, k in order:
            w_wait(layer, k, 1, s, sent=True)
            w_wait(layer, k, 2, end, sent=True)

        @pl.when(half == 0)
        def _():
            edge_copy.wait_send()

        final_arrived(1 - g)

    lane = lax.broadcasted_iota(jnp.int32, (128, 128), 1)
    line = lax.broadcasted_iota(jnp.int32, (128, 128), 0)

    @pl.loop(0, rows // 128)
    def _(b):
        at_rows = pl.ds(multiple(b * 128, 128), 128)
        summed = final[at_rows, :].astype(f32)
        mean = jnp.mean(summed, axis=1, keepdims=True)
        spread = jnp.mean(jnp.square(summed - mean), axis=1, keepdims=True)
        packed = jnp.where(lane == 0, mean, jnp.where(lane == 1, spread, 0.0))
        stats[t, :, at_rows] = packed.T[0:8, :]

    def stat_copy(k, owner):
        return copy(
            stats.at[owner], stats.at[owner], small_send.at[4 + k], small_recv.at[16 + k], (g, s, (t + k) % lanes)
        )

    for k in range(1, lanes):
        stat_copy(k, t).start()
    for k in range(1, lanes):
        stat_copy(k, (t + lanes - k) % lanes).wait()

    @pl.loop(0, rows // 128)
    def _(b):
        at_rows = pl.ds(multiple(b * 128, 128), 128)
        means = [stats[i, 0:1, at_rows] for i in range(lanes)]
        mean = sum(means) / lanes
        variance = sum(stats[i, 1:2, at_rows] + jnp.square(means[i] - mean) for i in range(lanes)) / lanes
        packed = jnp.where(line == 0, mean, jnp.where(line == 1, lax.rsqrt(variance + norm_eps), 0.0)).T
        centered = final[at_rows, :].astype(f32) - packed[:, 0:1]
        out[at_rows, :] = (
            centered * packed[:, 1:2] * ln_gain[LAYERS - 1 : LAYERS, :] + ln_bias[LAYERS - 1 : LAYERS, :]
        ).astype(bf16)


def mixer(tokens, proj_b, proj_c, proj_x, proj_out, conv_taps, ln_gain, ln_bias):
    parts, slabs, lanes = (lax.axis_size(a) for a in ("grp", "sp", "tp"))
    f32, bf16 = jnp.float32, jnp.bfloat16
    rows, ow = tokens.shape
    depth, channels = slabs * proj_b.shape[1], slabs * proj_out.shape[1]
    wide, owide = proj_b.shape[2] // parts, ow // parts
    total = parts * (HALO + 2 * rows)
    dma = pltpu.SemaphoreType.DMA
    anywhere, vmem = pl.BlockSpec(memory_space=pl.ANY), pl.BlockSpec(memory_space=pltpu.VMEM)
    return pl.pallas_call(
        mixer_kernel,
        out_shape=jax.ShapeDtypeStruct((rows, ow), bf16),
        in_specs=[anywhere] * 5 + [vmem] * 3,
        out_specs=vmem,
        scratch_shapes=[
            pltpu.VMEM((total, depth), bf16),
            pltpu.VMEM((total, depth), bf16),
            pltpu.VMEM((total, channels), bf16),
            pltpu.VMEM((LAYERS, depth, 3 * wide), bf16),
            pltpu.VMEM((LAYERS, channels, owide), bf16),
            pltpu.VMEM((total, 3 * wide), f32),
            pltpu.VMEM((8, wide), f32),
            pltpu.VMEM((4, rows, owide), bf16),
            pltpu.VMEM((rows, ow), bf16),
            pltpu.VMEM((8, depth), f32),
            pltpu.VMEM((8, ow), f32),
            pltpu.VMEM((lanes, 8, rows), f32),
            pltpu.VMEM((depth, 128), bf16),
            pltpu.VMEM((total // SUM_CHUNKS, 128), f32),
            dma((1 + 3 * LAYERS,)),
            dma((3, 3 * LAYERS)),
            dma((3, 3 * LAYERS)),
            dma((3, max(5, SUM_CHUNKS, BRANCH_CHUNKS), 7)),
            dma((3, max(5, SUM_CHUNKS, BRANCH_CHUNKS), 7)),
            dma((20,)),
            dma((20,)),
        ],
        compiler_params=pltpu.CompilerParams(
            has_side_effects=True, collective_id=0, vmem_limit_bytes=VMEM_BYTES
        ),
    )(tokens, proj_b, proj_c, proj_x, proj_out, conv_taps.transpose(1, 0, 2), ln_gain, ln_bias)


def solution(mesh):
    specs = dict(
        mesh=mesh,
        in_specs=(
            P(("grp", "sp"), "tp"),
            P(None, "sp", "tp"),
            P(None, "sp", "tp"),
            P(None, "sp", "tp"),
            P(None, "sp", "tp"),
            P(None, None, "tp"),
            P(None, "tp"),
            P(None, "tp"),
        ),
        out_specs=P(("grp", "sp"), "tp"),
        check_vma=False,
    )
    if (mesh.shape["grp"], mesh.shape["sp"], mesh.shape["tp"]) == (2, 4, 4):
        return jax.shard_map(mixer, **specs)
    return jax.shard_map(local, **specs)
```

```python
import jax
import jax.numpy as jnp
from jax import lax
from jax.experimental import pallas as pl
from jax.experimental.pallas import tpu as pltpu
from jax.sharding import PartitionSpec as P


LAYERS = 2


norm_eps = 1e-05


def from_behind(block, axis, distance):
    devices = range(lax.axis_size(axis))
    route = [(i - distance, i) for i in devices if i - distance in devices]
    return lax.ppermute(block, axis, route)


def along_line(block, axis, earlier):
    size = lax.axis_size(axis)
    blocks, latest = [(0, block)], []
    for side, step in enumerate((1, -1)):
        moving = block
        if earlier:
            moving, _ = lax.optimization_barrier((moving, earlier[side]))
        hops = []
        for hop in range(1, size):
            start = range(hop - 1, size - 1) if step == 1 else range(1, size - hop + 1)
            moving = lax.ppermute(moving, axis, [(i, i + step) for i in start])
            hops.append((-step * hop, moving))
        latest.append(hops[max(len(hops) - 2, 0)][1])
        blocks += hops
    return sorted(blocks, key=lambda b: abs(b[0])), latest


def dot_by_blocks(left, blocks, here, size):
    total = None
    for offset, block in blocks:
        depth = block.shape[0]
        owner = jnp.clip(here + offset, 0, size - 1)
        columns = lax.dynamic_slice_in_dim(left, owner * depth, depth, 1)
        term = jnp.dot(columns, block, preferred_element_type=jnp.float32)
        total = term if total is None else total + term
    return total


def local(tokens, proj_b, proj_c, proj_x, proj_out, conv_taps, ln_gain, ln_bias):
    residual_scale = (2.0 * LAYERS) ** 0.25
    parts = lax.axis_size("grp")
    me = lax.axis_index("grp")
    rows = tokens.shape[0]
    wide = proj_b.shape[2] // parts
    out_wide = proj_out.shape[2] // parts

    def mine(array, width):
        return lax.dynamic_slice_in_dim(array, me * width, width, array.ndim - 1)

    slabs, here = lax.axis_size("sp"), lax.axis_index("sp")
    weights = []
    earlier = None
    for layer_index in range(LAYERS):
        ins = jnp.concatenate(
            [mine(w[layer_index], wide) for w in (proj_b, proj_c, proj_x)], axis=1
        )
        ins, earlier = along_line(ins, "sp", earlier)
        outs, earlier = along_line(mine(proj_out[layer_index], out_wide), "sp", earlier)
        weights.append((ins, outs))
    taps, gain, bias = mine(conv_taps, wide), mine(ln_gain, out_wide), mine(ln_bias, out_wide)
    swapped = lax.all_to_all(
        tokens.reshape(rows, parts, out_wide), "grp", split_axis=1, concat_axis=0, tiled=False
    )
    hidden = swapped.reshape(parts * rows, out_wide)
    reach = taps.shape[1] - 1
    for layer_index in range(LAYERS):
        whole_in, whole_out = weights[layer_index]
        gathered = lax.all_gather(hidden, ("tp", "grp"), axis=1, tiled=True)
        acc = dot_by_blocks(gathered, whole_in, here, slabs)
        acc = lax.optimization_barrier(acc.astype(jnp.bfloat16)).astype(jnp.float32)
        out_gate, in_gate, values = (acc[:, i * wide : (i + 1) * wide] for i in range(3))
        gated_in = (in_gate * values).reshape(parts, rows, wide)
        fringe = from_behind(gated_in[:, rows - reach :], "sp", 1)
        padded = jnp.concatenate([fringe, gated_in], 1)
        conv_out = jnp.zeros_like(gated_in)
        for tap_index in range(reach + 1):
            conv_out = (
                conv_out + taps[layer_index, tap_index] * padded[:, tap_index : tap_index + rows]
            )
        branch = (out_gate * conv_out.reshape(parts * rows, wide)).astype(jnp.bfloat16)
        all_branch = lax.all_gather(branch, ("tp", "grp"), axis=1, tiled=True)
        acc_out = dot_by_blocks(all_branch, whole_out, here, slabs)
        mixed = lax.optimization_barrier(acc_out.astype(jnp.bfloat16))
        summed = residual_scale * hidden.astype(jnp.float32) + mixed.astype(jnp.float32)
        own_mean = jnp.mean(summed, axis=1)
        own_spread = jnp.mean(jnp.square(summed - own_mean[:, None]), axis=1)
        stats = lax.all_gather(jnp.stack([own_mean, own_spread]), ("tp", "grp"), axis=0)
        mean = jnp.mean(stats[:, 0], axis=0)
        variance = jnp.mean(stats[:, 1] + jnp.square(stats[:, 0] - mean), axis=0)[:, None]
        centered = summed - mean[:, None]
        hidden = (
            centered * lax.rsqrt(variance + norm_eps) * gain[layer_index] + bias[layer_index]
        ).astype(jnp.bfloat16)
    back = lax.all_to_all(
        hidden.reshape(parts, rows, out_wide), "grp", split_axis=0, concat_axis=1, tiled=False
    )
    return back.reshape(rows, parts * out_wide)


MESH = pl.DeviceIdType.MESH
BRANCH_CHUNKS = 5
SUM_CHUNKS = 5
BRANCH_AHEAD = 1
TOKEN_AHEAD = 1
OWN_HOOK = 2
OUT_EARLY = False
OUT_HOOK = 2
SUM_HOOK = 3
NEXT_HOOK = 2
SUM_AHEAD = 1
BRANCH_VIA_END = 1
SUM_VIA_END = 1
HALO = 32
VMEM_BYTES = 63 * 2**20


def multiple(value, of):
    return pl.multiple_of(value, of)


def tile_rows(rows, most):
    return max(n for n in range(16, most + 1, 16) if rows % n == 0)


def mixer_kernel(
    tokens, proj_b, proj_c, proj_x, proj_out, conv_taps, ln_gain, ln_bias, out,
    hidden, raw, branch, w_in, w_out, acc, carry, stage, final, scales, own_scales, stats, ones, means,
    local_sem, w_send, w_recv, ag_send, ag_recv, small_send, small_recv,
):
    f32, bf16 = jnp.float32, jnp.bfloat16
    residual_scale = (2.0 * LAYERS) ** 0.25
    g, s, t = (lax.axis_index(a) for a in ("grp", "sp", "tp"))
    parts, _, lanes = (lax.axis_size(a) for a in ("grp", "sp", "tp"))
    x, c = t // 2, t % 2
    rows, ow = tokens.shape
    kin, kout = proj_b.shape[1], proj_out.shape[1]
    wide, owide = proj_b.shape[2] // parts, ow // parts
    reach = conv_taps.shape[0] - 1
    part_rows = HALO + 2 * rows
    total = parts * part_rows
    half = s // 2
    base, end, mid = 2 * half, 3 * half, 1 + half
    other, far = 2 - half, 3 - 3 * half
    projections = (proj_b, proj_c, proj_x)
    kc = kin // 2
    pieces_in, pieces = (0, 1), 3

    def copy(src, dst, send, recv, device):
        return pltpu.make_async_remote_copy(src, dst, send, recv, device_id=device, device_id_type=MESH)

    def piece(layer, block, k):
        if k in pieces_in:
            return w_in.at[layer, pl.ds(multiple(block * kin + k * kc, kc), kc), :]
        return w_out.at[layer, pl.ds(multiple(block * kout, kout), kout), :]

    def piece_parts(layer, k):
        if k in pieces_in:
            columns = pl.ds(multiple(g * wide, wide), wide)
            rows_there = pl.ds(multiple(s * kin + k * kc, kc), kc)
            for j, w in enumerate(projections):
                yield w.at[layer, pl.ds(k * kc, kc), columns], w_in.at[layer, rows_there, pl.ds(j * wide, wide)]
        else:
            columns = pl.ds(multiple(g * owide, owide), owide)
            yield proj_out.at[layer, :, columns], piece(layer, s, k)

    def send_own(layer, k, device, row):
        sems = (w_send.at[row, layer * pieces + k], w_recv.at[row, layer * pieces + k])
        for src, dst in piece_parts(layer, k):
            copy(src, dst, *sems, device).start()

    def w_wait(layer, k, row, block, sent=False):
        ref = piece(layer, block, k)
        done = copy(ref, ref, w_send.at[row, layer * pieces + k], w_recv.at[row, layer * pieces + k], (g, s, t))
        done.wait_send() if sent else done.wait_recv()

    def relay(layer, k):
        w_wait(layer, k, 0, end)
        ref = piece(layer, end, k)
        sems = (w_send.at[2, layer * pieces + k], w_recv.at[2, layer * pieces + k])
        copy(ref, ref, *sems, (g, other, t)).start()

    order = [(layer, k) for layer in range(LAYERS) for k in range(pieces)]

    def token_rows(index):
        return pl.ds(multiple(g * part_rows + HALO + index * rows, 16), rows)

    def final_part(gg):
        return final.at[:, pl.ds(multiple(gg * owide, owide), owide)]

    def final_arrived(gg):
        ref = final_part(gg)
        copy(ref, ref, small_send.at[2], small_recv.at[8 + gg], (g, s, t)).wait_recv()

    yu, xu = g + c * (1 - 2 * g), x + (1 - c) * (1 - 2 * x)
    yv, xv = g + (1 - c) * (1 - 2 * g), x + c * (1 - 2 * x)
    up, vp, pp = (yu, s, 2 * xu + c), (yv, s, 2 * xv + c), (g, s, 2 * x + 1 - c)
    diagonal = (1 - g, s, 2 * (1 - x) + c)
    me = (g, s, t)

    def row_chunk(i, count):
        return pl.ds(multiple(i * (total // count), 16), total // count)

    def branch_columns(gg, tt):
        return pl.ds(multiple(tt * parts * wide + gg * wide, wide), wide)

    def branch_region(gg, tt, i):
        return row_chunk(i, BRANCH_CHUNKS), branch_columns(gg, tt)

    def sum_region(gg, tt, i):
        return row_chunk(i, SUM_CHUNKS), pl.ds(multiple(tt * ow + gg * owide, owide), owide)

    barrier = pltpu.get_barrier_semaphore()

    def greet(devices):
        for device in devices:
            pl.semaphore_signal(barrier, inc=1, device_id=device, device_id_type=MESH)
        pl.semaphore_wait(barrier, len(devices))

    lane_peers = [(g, s, (t + k) % lanes) for k in range(1, lanes)]

    def end_slab(j):
        start = multiple(g * part_rows + HALO + (end - base) * rows + j * (rows // 2), 16)
        return hidden.at[pl.ds(start, rows // 2), pl.ds(multiple(t * ow, ow), ow)]

    def end_tokens(j):
        return copy(
            tokens.at[pl.ds(j * (rows // 2), rows // 2), :], end_slab(j),
            small_send.at[3 * j], small_recv.at[3 * j], (g, mid, t),
        )

    @pl.when(s == end)
    def _():
        greet(lane_peers + [(1 - g, end, t)] + [(gg, mid, t) for gg in range(parts)])

        def send_tokens():
            for j in range(2):
                end_tokens(j).start()
            for j in range(2):
                end_tokens(j).wait_send()

        for layer, k in order:
            send_own(layer, k, (g, mid, t), 0)
            w_wait(layer, k, 0, s, sent=True)
            if (layer, k) == (0, 0):
                send_tokens()

        def pass_through(buffer, region, count, family, via):
            def transfer(owner, i, role, kind, device):
                ref = buffer.at[region(owner[0], owner[2], i)]
                return copy(ref, ref, ag_send.at[family, i, kind], ag_recv.at[family, i, role], device)

            through_end = range(count - via, count)
            for i in through_end:
                transfer(me, i, 3, 0, me).wait_recv()
                transfer(me, i, 0, 0, up).start()
                transfer(me, i, 1, 1, vp).start()
            for i in through_end:
                for role, owner in enumerate((up, vp, diagonal)):
                    transfer(me, i, role, 0, me).wait_recv()
                    if role == 0:
                        transfer(up, i, 2, 4, vp).start()
                    transfer(owner, i, role, (2, 3, 5)[role], (g, mid, t)).start()
            for i in through_end:
                for kind in range(6):
                    transfer(me, i, 0, kind, me).wait_send()

        pass_through(raw, sum_region, SUM_CHUNKS, 0, SUM_VIA_END)
        pass_through(branch, branch_region, BRANCH_CHUNKS, 2, BRANCH_VIA_END)
        for gg in range(parts):
            final_arrived(gg)

    @pl.when(s == mid)
    def _():
        there = (g, other, t)

        greet(lane_peers + [(1 - g, mid, t), there] + [(gg, end, t) for gg in range(parts)])
        send_own(0, 0, there, 1)
        mine = hidden.at[token_rows(mid - base), pl.ds(multiple(t * ow, ow), ow)]
        pltpu.make_async_copy(tokens, mine, local_sem.at[0]).start()
        for layer, k in order:
            for src, dst in piece_parts(layer, k):
                pltpu.make_async_copy(src, dst, local_sem.at[1 + layer * pieces + k]).start()

        edge = hidden.at[pl.ds(multiple(g * part_rows, 16), HALO), pl.ds(multiple(t * ow, ow), ow)]
        edge_copy = copy(tokens.at[pl.ds(rows - HALO, HALO), :], edge, small_send.at[1], small_recv.at[1], there)

        @pl.when(half == 0)
        def _():
            edge_copy.start()
            edge[...] = jnp.zeros_like(edge)

        own_scales[0:1, :] = ln_gain[0:1, :]
        own_scales[1:2, :] = ln_bias[0:1, :]
        scales[0:2, pl.ds(multiple(t * ow, ow), ow)] = own_scales[0:2, :]
        for k in range(1, lanes):
            copy(
                own_scales, scales.at[:, pl.ds(multiple(t * ow, ow), ow)],
                small_send.at[4 + k], small_recv.at[4 + k], (g, s, (t + k) % lanes),
            ).start()

        def gather(buffer, region, count, family, produce, consume, ahead, unroll=False, via=0, between=None, begun=0):
            def at(device, i):
                return buffer.at[region(device[0], device[2], i)]

            def transfer(owner, i, role, kind, device):
                ref = at(owner, i)
                return copy(ref, ref, ag_send.at[family, i, kind], ag_recv.at[family, i, role], device)

            def arrived(i, role):
                transfer(me, i, role, 0, me).wait_recv()

            def send(i):
                produce(i)
                transfer(me, i, 0, 0, up).start()
                transfer(me, i, 1, 1, vp).start()
                transfer(me, i, 3, 2, pp).start()

            def pass_on(i):
                arrived(i, 0)
                transfer(up, i, 2, 4, vp).start()
                transfer(up, i, 4, 3, pp).start()
                arrived(i, 1)
                transfer(vp, i, 5, 5, pp).start()

            def finish(i):
                arrived(i, 2)
                transfer(diagonal, i, 6, 6, pp).start()
                for role in range(3, 7):
                    arrived(i, role)
                consume(i)

            def sent(i, kinds):
                for kind in kinds:
                    transfer(me, i, 0, kind, me).wait_send()

            through_end = range(count - via, count)
            for i in through_end:
                produce(i)
                transfer(me, i, 3, 0, (g, end, t)).start()
                transfer(me, i, 3, 2, pp).start()
            count = count - via
            for i in range(begun, ahead):
                send(i)
            if unroll:
                for i in range(count + 1):
                    if i + ahead < count:
                        send(i + ahead)
                    if i < count:
                        pass_on(i)
                    if between:
                        between(i)
                    if i:
                        finish(i - 1)
            else:
                @pl.loop(0, count + 1)
                def _(i):
                    @pl.when(i + ahead < count)
                    def _():
                        send(i + ahead)

                    @pl.when(i < count)
                    def _():
                        pass_on(i)

                    @pl.when(i > 0)
                    def _():
                        finish(i - 1)

            for i in through_end:
                arrived(i, 0)
                transfer(up, i, 4, 3, pp).start()
                arrived(i, 1)
                transfer(vp, i, 5, 5, pp).start()
                finish(i)
                sent(i, (0, 2, 3, 5, 6))
            if unroll:
                for i in range(count):
                    sent(i, range(7))
            else:
                @pl.loop(0, count)
                def _(i):
                    sent(i, range(7))

        def nothing(i):
            pass

        first_half = rows // 2
        token_starts = (
            HALO + (mid - base) * rows,
            HALO + (mid - base) * rows + first_half,
            0,
            HALO + (end - base) * rows,
            HALO + (end - base) * rows + first_half,
        )

        def token_region(gg, tt, i):
            length = HALO if i == 2 else first_half
            return (
                pl.ds(multiple(gg * part_rows + token_starts[i], 16), length),
                pl.ds(multiple(tt * ow, ow), ow),
            )

        def token_ready(i):
            if i == 0:
                pltpu.make_async_copy(tokens, mine, local_sem.at[0]).wait()
            if i == 2:
                @pl.when(half == 1)
                def _():
                    edge_copy.wait_recv()
            if i > 2:
                slab = end_slab(i - 3)
                copy(slab, slab, small_send.at[3 * (i - 3)], small_recv.at[3 * (i - 3)], me).wait_recv()

        def token_hook(i):
            if i == 1:
                relay(0, 0)
            if i == OWN_HOOK:
                send_own(0, 1, there, 1)
            if i == 4:
                relay(0, 1)

        gather(hidden, token_region, 5, 0, token_ready, nothing, TOKEN_AHEAD, unroll=True, between=token_hook)

        def accumulate(layer, start, depth, at_rows, first=False):
            term = jnp.dot(
                hidden[at_rows, pl.ds(multiple(start, kc), depth)],
                w_in[layer, pl.ds(multiple(start, kc), depth), :],
                preferred_element_type=f32,
            )
            acc[at_rows, :] = term if first else acc[at_rows, :] + term

        def wait_near(layer, k):
            ref = piece(layer, s, k)
            pltpu.make_async_copy(ref, ref, local_sem.at[1 + layer * pieces + k]).wait()

        def near_in(layer, at_rows):
            accumulate(layer, base * kin, 2 * kin, at_rows, first=True)

        def far_in(layer):
            def add(start, depth):
                @pl.loop(0, 4)
                def _(i):
                    accumulate(layer, start, depth, row_chunk(i, 4))

            for k in pieces_in:
                w_wait(layer, k, 1, other)
            add(other * kin, kin)
            for k in pieces_in:
                w_wait(layer, k, 2, far)
                add(far * kin + k * kc, kc)

        tr = tile_rows(total // 10, 96)

        def gate(layer, i):
            taps = [
                conv_taps[n, layer : layer + 1, pl.ds(multiple(g * wide, wide), wide)] for n in range(reach + 1)
            ]
            row_of = lax.broadcasted_iota(jnp.int32, (tr, wide), 0)
            first = i * (total // BRANCH_CHUNKS)
            sums = acc[pl.ds(multiple(jnp.maximum(first - 8, 0), 8), 8), wide:].astype(bf16).astype(f32)
            unseen = HALO * (1 - half) - (first - 8) % part_rows
            carry[...] = jnp.where(row_of[:8] < unseen, 0.0, sums[:, :wide] * sums[:, wide:])

            @pl.loop(0, total // BRANCH_CHUNKS // tr)
            def _(q):
                start = multiple(i * (total // BRANCH_CHUNKS) + q * tr, 16)
                position = start % part_rows
                sums = acc[pl.ds(start, tr), :].astype(bf16).astype(f32)
                out_gate, in_gate, values = (sums[:, j * wide : (j + 1) * wide] for j in range(3))
                gated = in_gate * values
                gated = jnp.where(row_of < HALO * (1 - half) - position, 0.0, gated)
                before = jnp.where(position == 0, 0.0, carry[...])
                conv = jnp.zeros_like(gated)
                for n in range(reach + 1):
                    shift = reach - n
                    moved = gated
                    if shift:
                        moved = pltpu.roll(gated, shift, 0)
                        for j in range(shift):
                            moved = jnp.where(row_of == j, before[8 - shift + j : 8 - shift + j + 1, :], moved)
                    conv = conv + taps[n] * moved
                carry[...] = gated[tr - 8 :, :]
                branch[pl.ds(start, tr), branch_columns(g, t)] = (out_gate * conv).astype(bf16)

        def wait_out(layer):
            wait_near(layer, 2)
            for row, block in ((1, other), (2, far)):
                w_wait(layer, 2, row, block)

        own_columns = pl.ds(multiple(t * ow + g * owide, owide), owide)

        def mix(layer, at_rows):
            mixed = jnp.dot(branch[at_rows, :], w_out[layer], preferred_element_type=f32)
            kept = hidden[at_rows, own_columns].astype(f32)
            return (residual_scale * kept + mixed.astype(bf16).astype(f32)).astype(bf16)

        def produce_sum(i):
            at_rows = row_chunk(i, SUM_CHUNKS)
            raw[at_rows, own_columns] = mix(0, at_rows)

        strips = [slice(n, n + 128) for n in range(0, hidden.shape[1], 128)]
        ones[...] = jnp.ones_like(ones)

        def normalise(i):
            means[...] = jnp.dot(raw[row_chunk(i, SUM_CHUNKS), :], ones[...], preferred_element_type=f32) / ones.shape[0]

            @pl.loop(0, total // SUM_CHUNKS // tr)
            def _(q):
                there_rows = pl.ds(multiple(i * (total // SUM_CHUNKS) + q * tr, 16), tr)
                here_rows = pl.ds(multiple(q * tr, 16), tr)
                mean = means[here_rows, :]
                squares = jnp.zeros_like(mean)
                for strip in strips:
                    centered = raw[there_rows, strip].astype(f32) - mean
                    squares = squares + centered * centered
                scale = lax.rsqrt(jnp.sum(squares, axis=1, keepdims=True) / ones.shape[0] + norm_eps)
                scale = jnp.broadcast_to(scale, mean.shape)
                for strip in strips:
                    centered = raw[there_rows, strip].astype(f32) - mean
                    hidden[there_rows, strip] = (
                        centered * scale * scales[0:1, strip] + scales[1:2, strip]
                    ).astype(bf16)

        def send_pair(layer, k):
            send_own(layer, k, there, 1)
            relay(layer, k)

        def consume_sum(i):
            normalise(i)
            near_in(1, row_chunk(i, SUM_CHUNKS))

            @pl.when(i == OUT_HOOK)
            def _():
                send_pair(1, 2)

        def begin_sums():
            wait_out(0)
            produce_sum(0)
            ref = raw.at[sum_region(g, t, 0)]
            for role, kind, device in ((0, 0, up), (1, 1, vp), (3, 2, pp)):
                copy(ref, ref, ag_send.at[0, 0, kind], ag_recv.at[0, 0, role], device).start()

        def first_branches(i):
            @pl.when(i == SUM_HOOK)
            def _():
                begin_sums()

            @pl.when(i == BRANCH_CHUNKS - NEXT_HOOK)
            def _():
                send_pair(1, 0)

        for k in pieces_in:
            wait_near(0, k)

        @pl.loop(0, 4)
        def _(i):
            near_in(0, row_chunk(i, 4))

        if OUT_EARLY:
            send_pair(0, 2)
        far_in(0)
        if not OUT_EARLY:
            send_pair(0, 2)
        gather(
            branch, branch_region, BRANCH_CHUNKS, 1, lambda i: gate(0, i), first_branches, BRANCH_AHEAD
        )
        send_pair(1, 1)
        for k in range(1, lanes):
            copy(
                own_scales, scales.at[:, pl.ds(multiple(((t + lanes - k) % lanes) * ow, ow), ow)],
                small_send.at[4 + k], small_recv.at[4 + k], me,
            ).wait()
        for k in pieces_in:
            wait_near(1, k)
        gather(raw, sum_region, SUM_CHUNKS, 0, produce_sum, consume_sum, SUM_AHEAD, via=SUM_VIA_END, begun=1)
        far_in(1)
        gather(
            branch, branch_region, BRANCH_CHUNKS, 2, lambda i: gate(1, i), nothing, BRANCH_AHEAD,
            via=BRANCH_VIA_END,
        )
        wait_out(1)

        def result_copy(j):
            p = (g + 1 + j // 2) % 2
            to = end + (j % 2) * (mid - end)
            return p, to, copy(
                stage.at[j], final_part(g), small_send.at[12 + j], small_recv.at[8 + g], (p, to, t)
            )

        @pl.loop(0, 4)
        def _(j):
            p, to, result = result_copy(j)
            stage[j] = mix(1, pl.ds(multiple(p * part_rows + HALO + (to - base) * rows, 16), rows))

            @pl.when(j < 3)
            def _():
                result.start()

        final[:, pl.ds(multiple(g * owide, owide), owide)] = stage[3]
        for j in range(3):
            result_copy(j)[2].wait_send()
        for layer, k in order:
            w_wait(layer, k, 1, s, sent=True)
            w_wait(layer, k, 2, end, sent=True)

        @pl.when(half == 0)
        def _():
            edge_copy.wait_send()

        final_arrived(1 - g)

    lane = lax.broadcasted_iota(jnp.int32, (128, 128), 1)
    line = lax.broadcasted_iota(jnp.int32, (128, 128), 0)

    @pl.loop(0, rows // 128)
    def _(b):
        at_rows = pl.ds(multiple(b * 128, 128), 128)
        summed = final[at_rows, :].astype(f32)
        mean = jnp.mean(summed, axis=1, keepdims=True)
        spread = jnp.mean(jnp.square(summed - mean), axis=1, keepdims=True)
        packed = jnp.where(lane == 0, mean, jnp.where(lane == 1, spread, 0.0))
        stats[t, :, at_rows] = packed.T[0:8, :]

    def stat_copy(k, owner):
        return copy(
            stats.at[owner], stats.at[owner], small_send.at[4 + k], small_recv.at[16 + k], (g, s, (t + k) % lanes)
        )

    for k in range(1, lanes):
        stat_copy(k, t).start()
    for k in range(1, lanes):
        stat_copy(k, (t + lanes - k) % lanes).wait()

    @pl.loop(0, rows // 128)
    def _(b):
        at_rows = pl.ds(multiple(b * 128, 128), 128)
        means = [stats[i, 0:1, at_rows] for i in range(lanes)]
        mean = sum(means) / lanes
        variance = sum(stats[i, 1:2, at_rows] + jnp.square(means[i] - mean) for i in range(lanes)) / lanes
        packed = jnp.where(line == 0, mean, jnp.where(line == 1, lax.rsqrt(variance + norm_eps), 0.0)).T
        centered = final[at_rows, :].astype(f32) - packed[:, 0:1]
        out[at_rows, :] = (
            centered * packed[:, 1:2] * ln_gain[LAYERS - 1 : LAYERS, :] + ln_bias[LAYERS - 1 : LAYERS, :]
        ).astype(bf16)


def mixer(tokens, proj_b, proj_c, proj_x, proj_out, conv_taps, ln_gain, ln_bias):
    parts, slabs, lanes = (lax.axis_size(a) for a in ("grp", "sp", "tp"))
    f32, bf16 = jnp.float32, jnp.bfloat16
    rows, ow = tokens.shape
    depth, channels = slabs * proj_b.shape[1], slabs * proj_out.shape[1]
    wide, owide = proj_b.shape[2] // parts, ow // parts
    total = parts * (HALO + 2 * rows)
    dma = pltpu.SemaphoreType.DMA
    anywhere, vmem = pl.BlockSpec(memory_space=pl.ANY), pl.BlockSpec(memory_space=pltpu.VMEM)
    return pl.pallas_call(
        mixer_kernel,
        out_shape=jax.ShapeDtypeStruct((rows, ow), bf16),
        in_specs=[anywhere] * 5 + [vmem] * 3,
        out_specs=vmem,
        scratch_shapes=[
            pltpu.VMEM((total, depth), bf16),
            pltpu.VMEM((total, depth), bf16),
            pltpu.VMEM((total, channels), bf16),
            pltpu.VMEM((LAYERS, depth, 3 * wide), bf16),
            pltpu.VMEM((LAYERS, channels, owide), bf16),
            pltpu.VMEM((total, 3 * wide), f32),
            pltpu.VMEM((8, wide), f32),
            pltpu.VMEM((4, rows, owide), bf16),
            pltpu.VMEM((rows, ow), bf16),
            pltpu.VMEM((8, depth), f32),
            pltpu.VMEM((8, ow), f32),
            pltpu.VMEM((lanes, 8, rows), f32),
            pltpu.VMEM((depth, 128), bf16),
            pltpu.VMEM((total // SUM_CHUNKS, 128), f32),
            dma((1 + 3 * LAYERS,)),
            dma((3, 3 * LAYERS)),
            dma((3, 3 * LAYERS)),
            dma((3, max(5, SUM_CHUNKS, BRANCH_CHUNKS), 7)),
            dma((3, max(5, SUM_CHUNKS, BRANCH_CHUNKS), 7)),
            dma((20,)),
            dma((20,)),
        ],
        compiler_params=pltpu.CompilerParams(
            has_side_effects=True, collective_id=0, vmem_limit_bytes=VMEM_BYTES
        ),
    )(tokens, proj_b, proj_c, proj_x, proj_out, conv_taps.transpose(1, 0, 2), ln_gain, ln_bias)


def solution(mesh):
    specs = dict(
        mesh=mesh,
        in_specs=(
            P(("grp", "sp"), "tp"),
            P(None, "sp", "tp"),
            P(None, "sp", "tp"),
            P(None, "sp", "tp"),
            P(None, "sp", "tp"),
            P(None, None, "tp"),
            P(None, "tp"),
            P(None, "tp"),
        ),
        out_specs=P(("grp", "sp"), "tp"),
        check_vma=False,
    )
    if (mesh.shape["grp"], mesh.shape["sp"], mesh.shape["tp"]) == (2, 4, 4):
        return jax.shard_map(mixer, **specs)
    return jax.shard_map(local, **specs)
```
